512 devices in a mesh: sp: 64 (over z, y), tp: 8 (over x, core).
Axes of the slice: x: 4, y: 4, z: 16, core: 2. Of those that a mesh axis runs over, the one named last changes fastest.
Arguments:
- queries: bfloat16 [16384, 1024], P('sp', 'tp'), may hold values from -6 to 6
- keys: bfloat16 [16384, 512], P('sp', 'tp'), may hold values from -6 to 6
- values: bfloat16 [16384, 512], P('sp', 'tp'), may hold values from -6 to 6
- q_gain: float32 [64], replicated, may hold values from 1.6 to 4.5
- key_norm_gain: float32 [64], replicated, may hold values from 1.6 to 4.5
- out_weight: bfloat16 [1024, 2048], P('tp'), may hold values from -0.1875 to 0.1875
- residual: bfloat16 [16384, 2048], P('sp'), may hold values from -6 to 6
- ln1_gain: float32 [2048], replicated, may hold values from 0.1 to 1.9
- ln1_bias: float32 [2048], replicated, may hold values from -3 to 3
- up_weight: bfloat16 [2048, 8192], P('sp', 'tp'), may hold values from -0.125 to 0.125
- down_weight: bfloat16 [8192, 2048], P('tp', 'sp'), may hold values from -0.0625 to 0.0625
- ln2_gain: float32 [2048], replicated, may hold values from 0.1 to 1.9
- ln2_bias: float32 [2048], replicated, may hold values from -3 to 3
Outputs:
- encoded: bfloat16 [16384, 2048], P('sp', 'tp')
The draws below stay inside these ranges and needn't reach their ends.
All inputs are finite; a program needn't handle non-finite values.
Results may differ from the reference program's by a relative error of at most 0.014.
Values may be sent and summed in bfloat16 or wider, within the bound.
A program may use at most 64 MiB of HBM per device.

```python
import math
import jax
import jax.numpy as jnp
from jax import lax

D = 2048
FF = 8192
QUERY_HEADS = 16
KEY_VALUE_HEADS = 8
HEAD_SIZE = 64
GRID_W = 64
SEQUENCE_TOKENS = 16384
N_TP = 8


def random_base_keys(key):
    return jnp.clip(jax.random.normal(jax.random.fold_in(key, 11), (SEQUENCE_TOKENS, KEY_VALUE_HEADS * HEAD_SIZE), jnp.float32), -6.0, 6.0)


def draw_keys(key, part):
    return random_base_keys(key).astype(jnp.bfloat16)


def draw_queries(key, part):
    drawn_q = jnp.clip(jax.random.normal(jax.random.fold_in(key, 12), (SEQUENCE_TOKENS, QUERY_HEADS * HEAD_SIZE), jnp.float32), -6.0, 6.0)
    return drawn_q.astype(jnp.bfloat16)


def draw_q_gain(key, part):
    return jax.random.uniform(jax.random.fold_in(key, 21), (HEAD_SIZE,), jnp.float32, 1.6, 2.4)


def draw_key_norm_gain(key, part):
    return jax.random.uniform(jax.random.fold_in(key, 22), (HEAD_SIZE,), jnp.float32, 1.6, 2.4)


def block_levels(rng, extent, cuts, least, high):
    level, own = 1.0, jax.random.fold_in(rng, 6)
    for dim, blocks in cuts:
        heights = jnp.exp(jax.random.uniform(jax.random.fold_in(own, dim), (blocks,), jnp.float32, least / len(cuts), high / len(cuts)))
        level = level * jnp.repeat(heights, extent[dim] // blocks).reshape([-1 if axis == dim else 1 for axis in range(len(extent))])
    return level


def gaussian(key, extent, scale, limit, shards=(), kind=jnp.bfloat16):
    values = jax.random.normal(key, extent, jnp.float32) * scale
    if len(shards) > 0:
        values = block_levels(key, extent, shards, -0.22, 0.18) * values
    return jnp.clip(values, min=-limit, max=limit).astype(kind)


def setup_inputs(seed: int = 0) -> dict:
    key_list = jax.random.split(jax.random.key(seed), 14)
    return {
        "queries": draw_queries(jax.random.fold_in(key_list[13], 71), 0),
        "keys": draw_keys(jax.random.fold_in(key_list[13], 71), 0),
        "values": gaussian(key_list[2], (SEQUENCE_TOKENS, KEY_VALUE_HEADS * HEAD_SIZE), 1.0, 6.0, ((0, 64), (1, 8))),
        "q_gain": draw_q_gain(jax.random.fold_in(key_list[13], 71), 0),
        "key_norm_gain": draw_key_norm_gain(jax.random.fold_in(key_list[13], 71), 0),
        "out_weight": gaussian(key_list[5], (QUERY_HEADS * HEAD_SIZE, D), (QUERY_HEADS * HEAD_SIZE) ** -0.5, 0.1875, ((0, 8),)),
        "residual": gaussian(key_list[6], (SEQUENCE_TOKENS, D), 1.0, 6.0, ((0, 64),)),
        "ln1_gain": jnp.clip(1.0 + 0.18 * jax.random.normal(key_list[7], (D,), jnp.float32), 0.1, 1.9),
        "ln1_bias": gaussian(key_list[8], (D,), 0.3, 3.0, (), jnp.float32),
        "up_weight": gaussian(key_list[9], (D, FF), D ** -0.5, 0.125, ((0, 64), (1, 8))),
        "down_weight": gaussian(key_list[10], (FF, D), FF ** -0.5, 0.0625, ((0, 8), (1, 64))),
        "ln2_gain": jnp.clip(1.0 + 0.18 * jax.random.normal(key_list[11], (D,), jnp.float32), 0.1, 1.9),
        "ln2_bias": gaussian(key_list[12], (D,), 0.3, 3.0, (), jnp.float32),
    }


ALPHA = 8.0 ** 0.25
ROTARY_BASE = 10000.0
RMS_EPSILON = 1e-06
NORM_EPSILON = 1e-05

def rotate_grid(heads_in, grid_places):
    half_dim = heads_in.shape[-1] // 2
    quarter = half_dim // 2
    inverse = ROTARY_BASE ** (-jnp.arange(quarter, dtype=jnp.float32) / quarter)

    def spin(segment, coords):
        angles = coords.astype(jnp.float32)[:, None] * inverse[None, :]
        cos_val = jnp.cos(angles)[:, None, :]
        sin_val = jnp.sin(angles)[:, None, :]
        lead_half = segment[..., :quarter]
        tail_half = segment[..., quarter:]
        return jnp.concatenate([lead_half * cos_val - tail_half * sin_val, tail_half * cos_val + lead_half * sin_val], -1)
    return jnp.concatenate([spin(heads_in[..., :half_dim], grid_places // GRID_W), spin(heads_in[..., half_dim:], grid_places % GRID_W)], -1)

def prepare_inputs(heads_in, gain_vec, grid_places, factor):
    values32 = heads_in.astype(jnp.float32)
    normed = values32 * lax.rsqrt(lax.optimization_barrier(jnp.mean(values32 * values32, -1, keepdims=True)) + RMS_EPSILON) * gain_vec
    return (rotate_grid(normed, grid_places) * factor).astype(jnp.bfloat16)

def layer_norm(pre_norm, gain_vec, bias_vec):
    row_mean = lax.optimization_barrier(jnp.mean(pre_norm, -1, keepdims=True))
    centred = pre_norm - row_mean
    spread = lax.optimization_barrier(jnp.mean(centred * centred, -1, keepdims=True))
    return centred * lax.rsqrt(spread + NORM_EPSILON) * gain_vec + bias_vec

def sum_partials(left_side, right_side):
    group_width = left_side.shape[1] // N_TP
    totals = jnp.zeros((left_side.shape[0], right_side.shape[1]), jnp.float32)
    for member in range(N_TP):
        partial_value = jnp.dot(left_side[:, member * group_width:(member + 1) * group_width], right_side[member * group_width:(member + 1) * group_width], preferred_element_type=jnp.float32)
        totals = totals + lax.optimization_barrier(partial_value.astype(jnp.bfloat16)).astype(jnp.float32)
    return totals

def reference(queries, keys, values, q_gain, key_norm_gain, out_weight, residual, ln1_gain, ln1_bias, up_weight, down_weight, ln2_gain, ln2_bias):
    sequence_length = queries.shape[0]
    grid_places = jnp.arange(sequence_length, dtype=jnp.int32)
    group_count_size = QUERY_HEADS // KEY_VALUE_HEADS
    single_query_block = math.gcd(sequence_length, 128)
    query_head_rows = prepare_inputs(queries.reshape(sequence_length, QUERY_HEADS, HEAD_SIZE), q_gain, grid_places, HEAD_SIZE ** (-0.5))
    key_head_rows = prepare_inputs(keys.reshape(sequence_length, KEY_VALUE_HEADS, HEAD_SIZE), key_norm_gain, grid_places, 1.0).astype(jnp.float32)
    value_head_rows = values.reshape(sequence_length, KEY_VALUE_HEADS, HEAD_SIZE).astype(jnp.float32)
    query_block_list = query_head_rows.reshape(sequence_length // single_query_block, single_query_block, KEY_VALUE_HEADS, group_count_size, HEAD_SIZE)

    def attend(q_block):
        scores = jnp.einsum('qhgd,khd->hgqk', q_block.astype(jnp.float32), key_head_rows)
        maxima = lax.optimization_barrier(jnp.max(scores, -1, keepdims=True))
        weights = jnp.exp(scores - maxima)
        totals = lax.optimization_barrier(jnp.sum(weights, -1))
        rounded = lax.optimization_barrier(weights.astype(jnp.bfloat16)).astype(jnp.float32)
        summed = jnp.einsum('hgqk,khd->qhgd', rounded, value_head_rows)
        return summed / jnp.transpose(totals, (2, 0, 1))[..., None]
    attended = lax.map(attend, query_block_list).reshape(sequence_length, QUERY_HEADS * HEAD_SIZE).astype(jnp.bfloat16)
    mixed_sum = sum_partials(attended, out_weight)
    normed = layer_norm(ALPHA * residual.astype(jnp.float32) + mixed_sum, ln1_gain, ln1_bias).astype(jnp.bfloat16)
    up_acts = jnp.dot(normed, up_weight, preferred_element_type=jnp.float32)
    hidden = jnp.square(jnp.maximum(up_acts, 0.0)).astype(jnp.bfloat16)
    ffn_out = sum_partials(hidden, down_weight)
    return layer_norm(ALPHA * normed.astype(jnp.float32) + ffn_out, ln2_gain, ln2_bias).astype(jnp.bfloat16)
```

```python
import functools

import jax
import jax.numpy as jnp
import numpy as np
from jax import lax
from jax.experimental import pallas as pl
from jax.experimental.pallas import tpu as pltpu
from jax.sharding import PartitionSpec as P

HEAD = 64
GRID_W = 64
NY = 4
ALPHA = 8.0**0.25
ROTARY_BASE = 10000.0
RMS_EPSILON = 1e-06
NORM_EPSILON = 1e-05
LOG2E = 1.4426950408889634
ROWS = 256

f32, bf16 = jnp.float32, jnp.bfloat16


def rotary_tables(tokens):
    lane = np.arange(2 * HEAD) % HEAD
    pos = lane % 32
    freq = ROTARY_BASE ** (-(pos % 16) / 16.0)

    def table(count, mine):
        angle = np.arange(count)[:, None] * freq[None, :]
        cos, sin = np.cos(angle) * mine, np.sin(angle) * mine
        return np.concatenate([cos, np.where(pos < 16, -sin, 0.0), np.where(pos >= 16, sin, 0.0)], 1).astype(np.float32)

    return table(tokens // GRID_W, lane < 32), table(GRID_W, lane >= 32)


def dot(a, b, dims=((1,), (0,))):
    return lax.dot_general(a, b, (dims, ((), ())), preferred_element_type=f32)


NT = ((1,), (1,))


def kernel(
    NZ, NX, FA,
    q_ref, kv_ref, gq_ref, gk_ref, row_ref, col_ref, w_ref, wo_own, res_ref, g1_ref, b1_ref, g2_ref, b2_ref,
    out_ref,
    qb, kvb, qx, acc, mx, wb, wo, oms, omr, att, yb, res, xg, hid, part, prb, comb, rr, enc,
    q_s, q_r, kv_s, kv_r, wa_s, wa_r, wz_s, wz_r, ya_s, ya_r, yb_s, yb_r, wo_s, wo_r, wp_s, o_s, o_r, x_s, x_r, xp_s,
    p_s, p_r, r_s, r_r, e_s, e_r, loc,
):
    TP = 2 * NX
    HALF = NZ // 2
    sp, tp = lax.axis_index("sp"), lax.axis_index("tp")
    z, y = sp // NY, sp % NY
    x, core = tp // 2, tp % 2
    zr, zl = lax.rem(z + 1, NZ), lax.rem(z + NZ - 1, NZ)
    right, left = {"sp": zr * NY + y}, {"sp": zl * NY + y}
    partner = {"tp": x * 2 + 1 - core}
    me = y * TP + tp
    tok = q_ref.shape[0]
    own_rows = tok // TP
    D = wo.shape[2]

    def rc(src, dst, ss, rs, dev):
        return pltpu.make_async_remote_copy(
            src_ref=src, dst_ref=dst, send_sem=ss, recv_sem=rs, device_id=dev, device_id_type=pl.DeviceIdType.MESH
        )

    def got(ref, rs):
        rc(ref, ref, rs, rs, right).wait_recv()

    def sent(ref, ss):
        rc(ref, ref, ss, ss, right).wait_send()

    barrier = pltpu.get_barrier_semaphore()
    for dev in (right, left):
        pl.semaphore_signal(barrier, inc=1, device_id=dev, device_id_type=pl.DeviceIdType.MESH)

    @pl.loop(1, NY * TP)
    def _(i):
        d = lax.rem(me + i, NY * TP)
        pl.semaphore_signal(
            barrier, inc=1, device_id={"sp": z * NY + d // TP, "tp": lax.rem(d, TP)}, device_id_type=pl.DeviceIdType.MESH
        )

    res_copy = pltpu.make_async_copy(res_ref.at[pl.ds(tp * own_rows, own_rows), :], res, loc.at[0])
    res_copy.start()
    wo_copy = pltpu.make_async_copy(wo_own, wo.at[tp], loc.at[1])
    wo_copy.start()
    w_copy = pltpu.make_async_copy(w_ref, wb.at[sp], loc.at[2])
    w_copy.start()

    lane = lax.broadcasted_iota(jnp.int32, (1, 2 * HEAD), 1)
    low = lane < HEAD
    for r in range(tok // GRID_W):
        span = pl.ds(r * GRID_W, GRID_W)
        cs = [row_ref[r : r + 1, 128 * k : 128 * (k + 1)] + col_ref[:, 128 * k : 128 * (k + 1)] for k in range(3)]

        def turn(v, gain):
            sq = v * v
            s0 = jnp.sum(jnp.where(low, sq, 0.0), -1, keepdims=True)
            s1 = jnp.sum(jnp.where(low, 0.0, sq), -1, keepdims=True)
            inv = jnp.where(low, lax.rsqrt(s0 / HEAD + RMS_EPSILON), lax.rsqrt(s1 / HEAD + RMS_EPSILON))
            n = v * inv * gain
            return n * cs[0] + pltpu.roll(n, 112, 1) * cs[1] + pltpu.roll(n, 16, 1) * cs[2]

        qb[y, span, :] = turn(q_ref[span, :].astype(f32), gq_ref[...]).astype(bf16)
        kv = kv_ref[span, :].astype(f32)
        kvb[z, span, :] = jnp.where(low, turn(kv, gk_ref[...]), kv).astype(bf16)

    pl.semaphore_wait(barrier, NY * TP + 1)

    def send_kv(slot, to_right):
        if to_right:
            rc(kvb.at[slot], kvb.at[slot], kv_s.at[0, slot], kv_r.at[slot], right).start()
        else:
            rc(kvb.at[slot], kvb.at[slot], kv_s.at[1, slot], kv_r.at[slot], left).start()

    def wa_at(slot):
        return wb.at[pl.ds(slot * NY, NY), :, pl.ds(0, FA)]

    def wz_at(slot, row):
        return wb.at[slot * NY + row, :, pl.ds(FA, wb.shape[2] - FA)]

    def send_wa(slot, to_right):
        k, dev = (0, right) if to_right else (1, left)
        rc(wa_at(slot), wa_at(slot), wa_s.at[k, slot], wa_r.at[slot], dev).start()

    def send_wz(slot, to_right):
        k, dev = (0, right) if to_right else (1, left)
        rc(wz_at(slot, y), wz_at(slot, y), wz_s.at[k, slot], wz_r.at[slot], dev).start()

    def spread_wz(slot):
        for i in range(1, NY):
            t = lax.rem(y + i, NY)
            rc(wz_at(slot, y), wz_at(slot, y), yb_s.at[slot, i], yb_r.at[slot, y], {"sp": z * NY + t}).start()

    send_kv(z, True)
    send_kv(z, False)
    for i in range(1, NY):
        t = lax.rem(y + i, NY)
        rc(qb.at[y], qb.at[y], q_s.at[i], q_r.at[y], {"sp": z * NY + t}).start()
    w_copy.wait()
    for i in range(1, NY):
        t = lax.rem(y + i, NY)
        own = wb.at[sp, :, pl.ds(0, FA)]
        rc(own, own, ya_s.at[i], ya_r.at[y], {"sp": z * NY + t}).start()
    send_wz(z, True)
    send_wz(z, False)
    wo_copy.wait()
    for i in range(1, NX):
        t = lax.rem(x + i, NX) * 2 + core
        rc(wo.at[tp], wo.at[tp], wo_s.at[i], wo_r.at[tp], {"tp": t}).start()
    spread_wz(z)

    def spread_q(row):
        v = qb[row].astype(f32)
        h0 = jnp.where(low, v, 0.0).astype(bf16)
        h1 = jnp.where(low, pltpu.roll(v, HEAD, 1), 0.0).astype(bf16)
        for t in range(TP):
            at = (row * TP + t) * 2 * own_rows
            part_rows = slice(t * own_rows, (t + 1) * own_rows)
            qx[pl.ds(pl.multiple_of(at, own_rows), own_rows), :] = h0[part_rows]
            qx[pl.ds(pl.multiple_of(at + own_rows, own_rows), own_rows), :] = h1[part_rows]

    def flash(slots):
        kvs = [kvb[s] for s in slots]
        ones = [jnp.where(low, jnp.ones_like(k), k) for k in kvs]

        @pl.loop(0, qx.shape[0] // ROWS)
        def _(c):
            rows = pl.ds(pl.multiple_of(c * ROWS, ROWS), ROWS)
            qv = qx[rows, :]
            ss = [dot(qv, k, NT) for k in kvs]
            top = jnp.max(functools.reduce(jnp.maximum, ss), -1, keepdims=True)
            old = mx[rows, :]
            new = jnp.maximum(old, top)
            ps = [jnp.exp2(s - new[:, :1]).astype(bf16) for s in ss]
            add = functools.reduce(jnp.add, [dot(p, v) for p, v in zip(ps, ones)])
            acc[rows, :] = acc[rows, :] * jnp.exp2(old - new) + add
            mx[rows, :] = new

    acc[...] = jnp.zeros_like(acc)
    mx[...] = jnp.full_like(mx, -1e30)
    spread_q(y)
    for i in range(1, NY):
        t = lax.rem(y + i, NY)
        got(wb.at[z * NY + t, :, pl.ds(0, FA)], ya_r.at[t])
    send_wa(z, True)
    send_wa(z, False)
    for i in range(1, NY):
        t = lax.rem(y + i, NY)
        got(qb.at[t], q_r.at[t])
        spread_q(t)
    flash([z])

    @pl.loop(1, HALF)
    def _(s):
        a, b = lax.rem(z + NZ - s, NZ), lax.rem(z + s, NZ)
        more = s < HALF - 1
        got(kvb.at[a], kv_r.at[a])
        send_kv(a, True)
        got(kvb.at[b], kv_r.at[b])

        @pl.when(more)
        def _():
            send_kv(b, False)

        got(wz_at(a, y), wz_r.at[a])
        send_wz(a, True)
        got(wz_at(b, y), wz_r.at[b])

        @pl.when(more)
        def _():
            send_wz(b, False)

        got(wa_at(a), wa_r.at[a])
        send_wa(a, True)
        got(wa_at(b), wa_r.at[b])

        @pl.when(more)
        def _():
            send_wa(b, False)

        spread_wz(a)
        spread_wz(b)
        flash([a, b])

    far = lax.rem(z + HALF, NZ)
    got(kvb.at[far], kv_r.at[far])
    flash([far])

    @pl.loop(0, NY * TP)
    def _(i):
        d = lax.rem(me + 1 + i, NY * TP)
        span = pl.ds(pl.multiple_of(d * 2 * own_rows, 2 * own_rows), 2 * own_rows)
        a = acc[span, :]
        total = a[:, :1]
        lse = mx[span, :] + jnp.log2(total)
        hi = lse.astype(bf16).astype(f32)
        mid = (lse - hi).astype(bf16).astype(f32)
        sumparts = jnp.where(lane < 16, hi, jnp.where(lane < 32, mid, jnp.where(lane < 48, lse - hi - mid, 0.0)))
        message = jnp.where(low, sumparts, a / total).astype(bf16)

        @pl.when(d == me)
        def _():
            omr[me] = message

        @pl.when(d != me)
        def _():
            oms[d] = message
            rc(oms.at[d], omr.at[me], o_s.at[d], o_r.at[me], {"sp": z * NY + d // TP, "tp": lax.rem(d, TP)}).start()

    for i in range(1, NX):
        t = lax.rem(x + i, NX) * 2 + core
        got(wo.at[t], wo_r.at[t])
    for i in range(NX):
        t = lax.rem(x + i, NX) * 2 + core
        rc(wo.at[t], wo.at[t], wp_s.at[i], wo_r.at[t], partner).start()

    got(wz_at(far, y), wz_r.at[far])
    spread_wz(far)

    @pl.loop(1, NY * TP)
    def _(i):
        d = lax.rem(me + i, NY * TP)
        got(omr.at[d], o_r.at[d])

    @pl.loop(0, TP)
    def _(t):
        msgs = [omr[r * TP + t].astype(f32) for r in range(NY)]
        lses = [jnp.sum(jnp.where(lane < 48, m, 0.0), -1, keepdims=True) * (1.0 / 16.0) for m in msgs]
        top = functools.reduce(jnp.maximum, lses)
        ws = [jnp.exp2(v - top) for v in lses]
        o = functools.reduce(jnp.add, [w * m for w, m in zip(ws, msgs)]) / functools.reduce(jnp.add, ws)
        both = jnp.where(low, pltpu.roll(o[:own_rows], HEAD, 1), o[own_rows:])
        att[:, pl.ds(pl.multiple_of(t * 128, 128), 128)] = both.astype(bf16)

    for i in range(NX):
        t = lax.rem(x + i, NX) * 2 + 1 - core
        got(wo.at[t], wo_r.at[t])
    res_copy.wait()

    CW = 256

    @pl.loop(0, D // CW)
    def _(n):
        cols = pl.ds(pl.multiple_of(n * CW, CW), CW)
        w = wo[:, :, cols].reshape(TP * 128, CW)
        yb[:, cols] = dot(att[...], w) + ALPHA * res[:, cols].astype(f32)

    def norm(v, gain, bias):
        mean = jnp.mean(v, -1, keepdims=True)
        c = v - mean
        return c * lax.rsqrt(jnp.mean(c * c, -1, keepdims=True) + NORM_EPSILON) * gain + bias

    xg[tp] = norm(yb[...], g1_ref[...], b1_ref[...]).astype(bf16)
    for i in range(1, NX):
        t = lax.rem(x + i, NX) * 2 + core
        rc(xg.at[tp], xg.at[tp], x_s.at[i], x_r.at[tp], {"tp": t}).start()
    rc(xg.at[tp], xg.at[tp], xp_s.at[0], x_r.at[tp], partner).start()
    for i in range(1, NX):
        t = lax.rem(x + i, NX) * 2 + core
        got(xg.at[t], x_r.at[t])
        rc(xg.at[t], xg.at[t], xp_s.at[i], x_r.at[t], partner).start()

    got(wa_at(far), wa_r.at[far])

    @pl.loop(0, NZ)
    def _(s):
        for i in range(1, NY):
            t = lax.rem(y + i, NY)
            got(wz_at(s, t), yb_r.at[s, t])

    for i in range(NX):
        t = lax.rem(x + i, NX) * 2 + 1 - core
        got(xg.at[t], x_r.at[t])

    FW = wb.shape[2]
    piece = w_ref.shape[0] // 2
    per = 256 // piece

    @pl.loop(0, FW // CW)
    def _(n):
        cols = pl.ds(pl.multiple_of(n * CW, CW), CW)
        up = dot(xg[...].reshape(tok, D), wb[:, :piece, cols].reshape(D, CW))
        hid[:, cols] = jnp.square(jnp.maximum(up, 0.0)).astype(bf16)

    @pl.loop(0, D // 256)
    def _(n):
        w = wb[pl.ds(n * per, per), piece:, :].reshape(256, FW)
        ffn = dot(hid[...], w, NT).astype(bf16)
        part[:, :, pl.ds(pl.multiple_of(n * 256, 256), 256)] = ffn.reshape(TP, own_rows, 256)

    for i in range(NX):
        t = lax.rem(x + i, NX)
        rc(part.at[t * 2 + 1 - core], prb.at[t], p_s.at[i], p_r.at[t], partner).start()
    for i in range(1, NX):
        t = lax.rem(x + i, NX)
        got(prb.at[t], p_r.at[t])
        comb[t] = (part[t * 2 + core].astype(f32) + prb[t].astype(f32)).astype(bf16)
        rc(comb.at[t], rr.at[x], r_s.at[i], r_r.at[x], {"tp": t * 2 + core}).start()
    got(prb.at[x], p_r.at[x])
    yb[...] = part[tp].astype(f32) + prb[x].astype(f32) + ALPHA * xg[tp].astype(f32)
    for i in range(1, NX):
        t = lax.rem(x + i, NX)
        got(rr.at[t], r_r.at[t])
        yb[...] += rr[t].astype(f32)
    last = norm(yb[...], g2_ref[...], b2_ref[...]).astype(bf16)
    wide = D // TP
    for t in range(TP):
        enc[t] = last[:, t * wide : (t + 1) * wide]
    mine = pl.ds(tp * own_rows, own_rows)
    for i in range(1, TP):
        t = lax.rem(tp + i, TP)
        rc(enc.at[t], out_ref.at[mine, :], e_s.at[i], e_r.at[tp], {"tp": t}).start()
    out_ref[mine, :] = enc[tp]
    for i in range(1, TP):
        t = lax.rem(tp + i, TP)
        got(out_ref.at[pl.ds(t * own_rows, own_rows), :], e_r.at[t])

    for i in range(1, NY):
        sent(qb.at[y], q_s.at[i])
        sent(wb.at[sp, :, pl.ds(0, FA)], ya_s.at[i])
    for i in range(1, NX):
        sent(wo.at[tp], wo_s.at[i])
        sent(xg.at[tp], x_s.at[i])
        sent(comb.at[0], r_s.at[i])
    for i in range(NX):
        sent(wo.at[tp], wp_s.at[i])
        sent(xg.at[tp], xp_s.at[i])
        sent(part.at[0], p_s.at[i])
    for i in range(1, TP):
        sent(enc.at[0], e_s.at[i])

    @pl.loop(1, NY * TP)
    def _(i):
        d = lax.rem(me + i, NY * TP)
        sent(oms.at[d], o_s.at[d])

    @pl.loop(0, NZ)
    def _(s):
        for i in range(1, NY):
            sent(wz_at(s, y), yb_s.at[s, i])

    @pl.loop(0, HALF)
    def _(s):
        a, b = lax.rem(z + NZ - s, NZ), lax.rem(z + s, NZ)
        sent(kvb.at[a], kv_s.at[0, a])
        sent(wa_at(a), wa_s.at[0, a])
        sent(wz_at(a, y), wz_s.at[0, a])

        @pl.when(s < HALF - 1)
        def _():
            sent(kvb.at[b], kv_s.at[1, b])
            sent(wa_at(b), wa_s.at[1, b])
            sent(wz_at(b, y), wz_s.at[1, b])


def solution(mesh):
    SP, TP = mesh.shape["sp"], mesh.shape["tp"]
    NZ, NX = SP // NY, TP // 2

    def local(queries, keys, values, q_gain, key_norm_gain, out_weight, residual, ln1_gain, ln1_bias, up_weight, down_weight, ln2_gain, ln2_bias):
        tok, D, FW = queries.shape[0], out_weight.shape[1], up_weight.shape[1]
        own = tok // TP
        FA = (FW // 128 * 3 // 8) * 128
        piece = up_weight.shape[0]
        rows, cols = rotary_tables(tok * SP)
        per = tok // GRID_W
        rows = lax.dynamic_slice_in_dim(jnp.asarray(rows), lax.axis_index("sp") * per, per, 0)
        kv = jnp.concatenate([keys, values], axis=1)
        w = jnp.concatenate([up_weight, down_weight.T], axis=0)
        gq = jnp.tile(q_gain * (HEAD**-0.5 * LOG2E), 2)[None, :]
        gk = jnp.concatenate([key_norm_gain, jnp.ones_like(key_norm_gain)])[None, :]
        vm, hbm = pl.BlockSpec(memory_space=pltpu.VMEM), pl.BlockSpec(memory_space=pl.ANY)
        dma = pltpu.SemaphoreType.DMA
        V = pltpu.VMEM
        flops = 2 * tok * tok * SP * 256 + 4 * tok * D * FW
        return pl.pallas_call(
            functools.partial(kernel, NZ, NX, FA),
            out_shape=jax.ShapeDtypeStruct((tok, D // TP), bf16),
            in_specs=[vm, vm, vm, vm, vm, vm, hbm, hbm, hbm, vm, vm, vm, vm],
            out_specs=vm,
            scratch_shapes=[
                V((NY, tok, 128), bf16), V((NZ, tok, 128), bf16), V((NY * tok * 2, 128), bf16),
                V((NY * tok * 2, 128), f32), V((NY * tok * 2, 128), f32),
                V((SP, 2 * piece, FW), bf16), V((TP, 128, D), bf16),
                V((NY * TP, 2 * own, 128), bf16), V((NY * TP, 2 * own, 128), bf16), V((own, TP * 128), bf16),
                V((own, D), f32), V((own, D), bf16), V((TP, own, D), bf16), V((tok, FW), bf16), V((TP, own, D), bf16),
                V((NX, own, D), bf16), V((NX, own, D), bf16), V((NX, own, D), bf16), V((TP, own, D // TP), bf16),
                dma((NY,)), dma((NY,)), dma((2, NZ)), dma((NZ,)), dma((2, NZ)), dma((NZ,)), dma((2, NZ)), dma((NZ,)),
                dma((NY,)), dma((NY,)), dma((NZ, NY)), dma((NZ, NY)), dma((NX,)), dma((TP,)), dma((NX,)),
                dma((NY * TP,)), dma((NY * TP,)), dma((NX,)), dma((TP,)), dma((NX,)),
                dma((NX,)), dma((NX,)), dma((NX,)), dma((NX,)), dma((TP,)), dma((TP,)), dma((3,)),
            ],
            compiler_params=pltpu.CompilerParams(collective_id=0, has_side_effects=True, vmem_limit_bytes=60000000),
            cost_estimate=pl.CostEstimate(flops=flops, bytes_accessed=30000000, transcendentals=0),
        )(queries, kv, gq, gk, rows, jnp.asarray(cols), w, out_weight, residual, ln1_gain[None], ln1_bias[None], ln2_gain[None], ln2_bias[None])

    return jax.shard_map(
        local,
        mesh=mesh,
        in_specs=(
            P("sp", "tp"), P("sp", "tp"), P("sp", "tp"), P(), P(), P("tp", None), P("sp", None),
            P(), P(), P("sp", "tp"), P("tp", "sp"), P(), P(),
        ),
        out_specs=P("sp", "tp"),
        check_vma=False,
    )
```

```python
import functools

import jax
import jax.numpy as jnp
import numpy as np
from jax import lax
from jax.experimental import pallas as pl
from jax.experimental.pallas import tpu as pltpu
from jax.sharding import PartitionSpec as P

HEAD = 64
GRID_W = 64
NY = 4
ALPHA = 8.0**0.25
ROTARY_BASE = 10000.0
RMS_EPSILON = 1e-06
NORM_EPSILON = 1e-05
LOG2E = 1.4426950408889634
f32, bf16 = jnp.float32, jnp.bfloat16


def rotary_tables(tokens, devices):
    lane = np.arange(2 * HEAD) % HEAD
    pos = lane % 32
    freq = ROTARY_BASE ** (-(pos % 16) / 16.0)

    def table(count, mine):
        angle = np.arange(count)[:, None] * freq[None, :]
        cos, sin = np.cos(angle) * mine, np.sin(angle) * mine
        return np.concatenate([cos, np.where(pos < 16, -sin, 0.0), np.where(pos >= 16, sin, 0.0)], 1).astype(np.float32)

    rows = table(tokens // GRID_W, lane < 32).reshape(devices, -1, 6 * HEAD)
    return np.pad(rows, ((0, 0), (0, -rows.shape[1] % 8), (0, 0))), table(GRID_W, lane >= 32)


def dot(a, b, dims=((1,), (0,))):
    return lax.dot_general(a, b, (dims, ((), ())), preferred_element_type=f32)


NT = ((1,), (1,))


def kernel(
    NZ, NX, FA,
    q_ref, k_ref, v_ref, gq_ref, gk_ref, row_ref, col_ref, up_ref, down_ref, wo_own, res_ref, g1_ref, b1_ref, g2_ref, b2_ref,
    out_ref,
    rowv, qb, kvb, qx, acc, mx, wb, wo, oms, omr, att, yb, res, xg, hid, part, prb, comb, rr, enc,
    q_s, q_r, kv_s, kv_r, wa_s, wa_r, wz_s, wz_r, ya_s, ya_r, yf_s, yf_r, yh_r, wo_s, wo_r, wp_s, o_s, o_r, x_s, x_r, xp_s,
    p_s, p_r, r_s, r_r, e_s, e_r, loc,
):
    TP = 2 * NX
    HALF = NZ // 2
    sp, tp = lax.axis_index("sp"), lax.axis_index("tp")
    z, y = sp // NY, lax.rem(sp, NY)
    x, core = tp // 2, lax.rem(tp, 2)
    zr, zl = lax.rem(z + 1, NZ), lax.rem(z + NZ - 1, NZ)
    yu, yd = lax.rem(y + 1, NY), lax.rem(y + NY - 1, NY)
    right, left = {"sp": zr * NY + y}, {"sp": zl * NY + y}
    above, below = {"sp": z * NY + yu}, {"sp": z * NY + yd}
    partner = {"tp": x * 2 + 1 - core}
    me = y * TP + tp
    tok = q_ref.shape[0]
    own_rows = tok // TP
    D = wo.shape[2]
    FW = wb.shape[2]
    piece = up_ref.shape[0]

    def rc(src, dst, ss, rs, dev):
        return pltpu.make_async_remote_copy(
            src_ref=src, dst_ref=dst, send_sem=ss, recv_sem=rs, device_id=dev, device_id_type=pl.DeviceIdType.MESH
        )

    def got(ref, rs):
        rc(ref, ref, rs, rs, right).wait_recv()

    def sent(ref, ss):
        rc(ref, ref, ss, ss, right).wait_send()

    barrier = pltpu.get_barrier_semaphore()
    for dev in (right, left):
        pl.semaphore_signal(barrier, inc=1, device_id=dev, device_id_type=pl.DeviceIdType.MESH)

    @pl.loop(1, NY * TP)
    def _(i):
        d = lax.rem(me + i, NY * TP)
        pl.semaphore_signal(
            barrier, inc=1, device_id={"sp": z * NY + d // TP, "tp": lax.rem(d, TP)}, device_id_type=pl.DeviceIdType.MESH
        )

    copies = [
        pltpu.make_async_copy(row_ref.at[sp], rowv, loc.at[0]),
        pltpu.make_async_copy(up_ref, wb.at[sp, pl.ds(0, piece), :], loc.at[1]),
        pltpu.make_async_copy(down_ref, wb.at[sp, pl.ds(piece, piece), :], loc.at[2]),
        pltpu.make_async_copy(wo_own, wo.at[tp], loc.at[3]),
        pltpu.make_async_copy(res_ref.at[pl.ds(tp * own_rows, own_rows), :], res, loc.at[4]),
    ]
    for c in copies:
        c.start()

    lane = lax.broadcasted_iota(jnp.int32, (1, 2 * HEAD), 1)
    low = lane < HEAD
    kv_all = jnp.transpose(jnp.concatenate([k_ref[...].astype(f32), v_ref[...].astype(f32)], 0))
    gq = jnp.concatenate([gq_ref[...], gq_ref[...]], 1) * (HEAD**-0.5 * LOG2E)
    gk = jnp.concatenate([gk_ref[...], gk_ref[...]], 1)
    copies[0].wait()

    def spans():
        for r in range(tok // GRID_W):
            cs = [rowv[r : r + 1, 128 * k : 128 * (k + 1)] + col_ref[:, 128 * k : 128 * (k + 1)] for k in range(3)]
            yield pl.ds(r * GRID_W, GRID_W), cs, kv_all[r * GRID_W : (r + 1) * GRID_W]

    def turn(v, gain, cs):
        sq = v * v
        s0 = jnp.sum(jnp.where(low, sq, 0.0), -1, keepdims=True)
        s1 = jnp.sum(jnp.where(low, 0.0, sq), -1, keepdims=True)
        inv = jnp.where(low, lax.rsqrt(s0 / HEAD + RMS_EPSILON), lax.rsqrt(s1 / HEAD + RMS_EPSILON))
        n = v * inv * gain
        return n * cs[0] + pltpu.roll(n, 112, 1) * cs[1] + pltpu.roll(n, 16, 1) * cs[2]

    for span, cs, kv in spans():
        kvb[z, span, :] = jnp.where(low, turn(kv, gk, cs), kv).astype(bf16)

    pl.semaphore_wait(barrier, NY * TP + 1)

    def wa_at(slot, k):
        return wb.at[pl.ds(slot * NY + k * (NY // 2), NY // 2), :, pl.ds(0, FA)]

    def wz_at(slot, row):
        return wb.at[slot * NY + row, :, pl.ds(FA, FW - FA)]

    def half_at(slot, row, k):
        return wb.at[slot * NY + row, pl.ds(k * piece, piece), pl.ds(FA, FW - FA)]

    def send_kv(slot, dev):
        rc(kvb.at[slot], kvb.at[slot], kv_s, kv_r.at[slot], dev).start()

    def send_wa(slot, dev, k):
        rc(wa_at(slot, k), wa_at(slot, k), wa_s, wa_r.at[slot, k], dev).start()

    def send_wz(slot, dev):
        rc(wz_at(slot, y), wz_at(slot, y), wz_s, wz_r.at[slot], dev).start()

    def minus(s):
        return lax.rem(z + NZ - s, NZ)

    def plus(s):
        return lax.rem(z + s, NZ)

    def both(s, ref, sem, send, send_first, send_last):
        def onward():
            send(minus(s), right)

        def last():
            send_first(minus(s), right)

        got(ref(minus(s)), sem.at[minus(s)])
        if isinstance(s, int):
            onward() if s < HALF - 1 else last()
        else:
            pl.when(s < HALF - 1)(onward)
            pl.when(s == HALF - 1)(last)
        got(ref(plus(s)), sem.at[plus(s)])
        if isinstance(s, int):
            send(plus(s), left) if s < HALF - 1 else send_last(plus(s), left)
        else:
            pl.when(s < HALF - 1)(lambda: send(plus(s), left))
            pl.when(s == HALF - 1)(lambda: send_last(plus(s), left))

    def step_kv(s):
        def part_of(lo):
            def f(i, dev):
                r = kvb.at[i, pl.ds(lo, tok // 2), :]
                rc(r, r, kv_s, kv_r.at[i], dev).start()

            return f

        both(s, lambda i: kvb.at[i], kv_r, send_kv, part_of(0), part_of(tok // 2))

    def step_wz(s):
        def part_of(k):
            def f(i, dev):
                rc(half_at(i, y, k), half_at(i, y, k), wz_s, wz_r.at[i], dev).start()

            return f

        both(s, lambda i: wz_at(i, y), wz_r, send_wz, part_of(0), part_of(1))

    def step_wa(s):
        for k in range(2):

            def nothing(i, dev):
                pass

            def go(i, dev, k=k):
                send_wa(i, dev, k)

            both(s, lambda i, k=k: wa_at(i, k), wa_r.at[:, k], go, go if k == 0 else nothing, go if k == 1 else nothing)

    def spread(slot):
        rc(wz_at(slot, y), wz_at(slot, y), yf_s, yf_r.at[slot, 0], above).start()
        rc(wz_at(slot, y), wz_at(slot, y), yf_s, yf_r.at[slot, 1], below).start()

    def relay(slot):
        got(wz_at(slot, yd), yf_r.at[slot, 0])
        rc(half_at(slot, yd, 0), half_at(slot, yd, 0), yf_s, yh_r, above).start()
        got(wz_at(slot, yu), yf_r.at[slot, 1])
        rc(half_at(slot, yu, 1), half_at(slot, yu, 1), yf_s, yh_r, below).start()

    def pair(s, f):
        f(minus(s))
        f(plus(s))

    send_kv(z, right)
    send_kv(z, left)
    copies[1].wait()
    copies[2].wait()
    for i in range(1, NY):
        t = lax.rem(y + i, NY)
        own = wb.at[sp, :, pl.ds(0, FA)]
        rc(own, own, ya_s, ya_r.at[y], {"sp": z * NY + t}).start()
    send_wz(z, right)
    send_wz(z, left)
    for span, cs, kv in spans():
        qb[y, span, :] = turn(q_ref[span, :].astype(f32), gq, cs).astype(bf16)
    for i in range(1, NY):
        t = lax.rem(y + i, NY)
        rc(qb.at[y], qb.at[y], q_s, q_r.at[y], {"sp": z * NY + t}).start()
    spread(z)
    copies[3].wait()
    for i in range(1, NX):
        t = lax.rem(x + i, NX) * 2 + core
        rc(wo.at[tp], wo.at[tp], wo_s, wo_r.at[0], {"tp": t}).start()

    def spread_q(row):
        v = qb[row].astype(f32)
        h0 = jnp.where(low, v, 0.0).astype(bf16)
        h1 = jnp.where(low, pltpu.roll(v, HEAD, 1), 0.0).astype(bf16)
        for t in range(TP):
            at = (row * TP + t) * 2 * own_rows
            part_rows = slice(t * own_rows, (t + 1) * own_rows)
            qx[pl.ds(pl.multiple_of(at, own_rows), own_rows), :] = h0[part_rows]
            qx[pl.ds(pl.multiple_of(at + own_rows, own_rows), own_rows), :] = h1[part_rows]

    def flash(slots):
        kvs = [kvb[s] for s in slots]
        ones = [jnp.where(low, jnp.ones_like(k), k) for k in kvs]
        ss = [dot(qx[...], k, NT) for k in kvs]
        top = jnp.max(functools.reduce(jnp.maximum, ss), -1, keepdims=True)
        old = mx[...]
        new = jnp.maximum(old, top)
        wide = jnp.concatenate([new] * (tok // 128), 1) if tok > 128 else new[:, :tok]
        ps = [jnp.exp2(s - wide).astype(bf16) for s in ss]
        add = functools.reduce(jnp.add, [dot(p, v) for p, v in zip(ps, ones)])
        acc[...] = acc[...] * jnp.exp2(old - new) + add
        mx[...] = new

    acc[...] = jnp.zeros_like(acc)
    mx[...] = jnp.full_like(mx, -1e30)
    spread_q(y)
    NA = (HALF - 1) // 3
    SM = HALF - 3

    @pl.loop(1, HALF)
    def _(s):
        step_kv(s)
        step_wz(s)

        @pl.when(s == 1)
        def _():
            for i in range(1, NY):
                t = lax.rem(y + i, NY)
                got(wb.at[z * NY + t, :, pl.ds(0, FA)], ya_r.at[t])
            for k in range(2):
                send_wa(z, right, k)
                send_wa(z, left, k)
            for i in range(1, NY):
                t = lax.rem(y + i, NY)
                got(qb.at[t], q_r.at[t])
                spread_q(t)
            flash([z])

        @pl.when(lax.rem(s, 3) == 0)
        def _():
            step_wa(s // 3)

        @pl.when(s <= SM)
        def _():
            pair(s, spread)

        flash([minus(s), plus(s)])

        @pl.when(s <= SM + 1)
        def _():
            relay(minus(s - 1))

            @pl.when(s > 1)
            def _():
                relay(plus(s - 1))

    far = lax.rem(z + HALF, NZ)
    got(kvb.at[far], kv_r.at[far])
    flash([far])

    total = pltpu.roll(acc[...], HEAD, 1)
    lse = mx[...] + jnp.log2(acc[...])
    hi = lse.astype(bf16).astype(f32)
    mid = (lse - hi).astype(bf16).astype(f32)
    sumparts = jnp.where(lane < 16, hi, jnp.where(lane < 32, mid, jnp.where(lane < 48, lse - hi - mid, 0.0)))
    oms[...] = jnp.where(low, sumparts, acc[...] / total).astype(bf16).reshape(oms.shape)

    @pl.loop(1, NY * TP)
    def _(i):
        d = lax.rem(me + i, NY * TP)
        rc(oms.at[d], omr.at[me], o_s, o_r, {"sp": z * NY + d // TP, "tp": lax.rem(d, TP)}).start()

    omr[me] = oms[me]
    for s in range(SM + 1, HALF):
        pair(s, spread)
    step_wa(NA + 1)
    if NX > 1:
        got(wo.at[pl.ds(0, NX - 1)], wo_r.at[0])
    for i in range(NX):
        t = lax.rem(x + i, NX) * 2 + core
        rc(wo.at[t], wo.at[t], wp_s, wo_r.at[1], partner).start()
    got(wz_at(far, y), wz_r.at[far])
    spread(far)
    mid_a = min(NA + 3, HALF - 1)
    for s in range(NA + 2, mid_a + 1):
        step_wa(s)
    got(omr.at[pl.ds(0, NY * TP - 1)], o_r)

    @pl.loop(0, TP)
    def _(t):
        msgs = [omr[r * TP + t].astype(f32) for r in range(NY)]
        lses = [jnp.sum(jnp.where(lane < 48, m, 0.0), -1, keepdims=True) * (1.0 / 16.0) for m in msgs]
        top = functools.reduce(jnp.maximum, lses)
        ws = [jnp.exp2(v - top) for v in lses]
        o = functools.reduce(jnp.add, [w * m for w, m in zip(ws, msgs)]) / functools.reduce(jnp.add, ws)
        heads = jnp.where(low, pltpu.roll(o[:own_rows], HEAD, 1), o[own_rows:])
        att[:, pl.ds(pl.multiple_of(t * 128, 128), 128)] = heads.astype(bf16)

    got(wo.at[pl.ds(0, NX)], wo_r.at[1])
    copies[4].wait()

    CW = 256

    @pl.loop(0, D // CW)
    def _(n):
        cols = pl.ds(pl.multiple_of(n * CW, CW), CW)
        w = wo[:, :, cols].reshape(TP * 128, CW)
        yb[:, cols] = dot(att[...], w) + ALPHA * res[:, cols].astype(f32)

    def norm(v, gain, bias):
        mean = jnp.mean(v, -1, keepdims=True)
        c = v - mean
        return c * lax.rsqrt(jnp.mean(c * c, -1, keepdims=True) + NORM_EPSILON) * gain + bias

    xg[tp] = norm(yb[...], g1_ref[...], b1_ref[...]).astype(bf16)
    for i in range(1, NX):
        t = lax.rem(x + i, NX) * 2 + core
        rc(xg.at[tp], xg.at[tp], x_s, x_r.at[tp], {"tp": t}).start()
    rc(xg.at[tp], xg.at[tp], xp_s, x_r.at[TP], partner).start()
    late = list(range(SM + 1, HALF))
    for s in range(mid_a + 1, HALF):
        step_wa(s)
        if late:
            pair(late.pop(0), relay)
    for i in range(1, NX):
        t = lax.rem(x + i, NX) * 2 + core
        got(xg.at[t], x_r.at[t])
        rc(xg.at[t], xg.at[t], xp_s, x_r.at[TP], partner).start()

    for s in late:
        pair(s, relay)
    relay(far)
    for k in range(2):
        got(wa_at(far, k), wa_r.at[far, k])
    got(xg.at[pl.ds(0, NX)], x_r.at[TP])
    got(wb.at[pl.ds(0, NZ), :, pl.ds(FA, FW - FA)], yh_r)

    @pl.loop(0, FW // CW)
    def _(n):
        cols = pl.ds(pl.multiple_of(n * CW, CW), CW)
        up = dot(xg[...].reshape(tok, D), wb[:, :piece, cols].reshape(D, CW))
        hid[:, cols] = jnp.square(jnp.maximum(up, 0.0)).astype(bf16)

    QW = part.shape[3]
    quarters = D // QW
    nb = min(256, QW)
    per = nb // piece

    def down(h):
        @pl.loop(0, QW // nb)
        def _(n):
            w = wb[pl.ds((h * (QW // nb) + n) * per, per), piece:, :].reshape(nb, FW)
            ffn = dot(hid[...], w, NT).astype(bf16)
            part[h, :, :, pl.ds(pl.multiple_of(n * nb, nb), nb)] = ffn.reshape(TP, own_rows, nb)

        for i in range(1, NX + 1):
            t = lax.rem(x + i, NX)
            rc(part.at[h, t * 2 + 1 - core], prb.at[h, t], p_s, p_r.at[h], partner).start()

    def fold(h):
        got(prb.at[h], p_r.at[h])
        for i in range(1, NX):
            t = lax.rem(x + i, NX)
            comb[h, t] = (part[h, t * 2 + core].astype(f32) + prb[h, t].astype(f32)).astype(bf16)
            rc(comb.at[h, t], rr.at[h, x], r_s, r_r.at[h], {"tp": t * 2 + core}).start()

    for h in range(quarters):
        down(h)
        if h > 0:
            fold(h - 1)
    fold(quarters - 1)
    for h in range(quarters):
        cols = slice(h * QW, (h + 1) * QW)
        total = part[h, tp].astype(f32) + prb[h, x].astype(f32) + ALPHA * xg[tp, :, cols].astype(f32)
        if NX > 1:
            got(rr.at[h, pl.ds(0, NX - 1)], r_r.at[h])
            for i in range(1, NX):
                total += rr[h, lax.rem(x + i, NX)].astype(f32)
        yb[:, cols] = total
    last = norm(yb[...], g2_ref[...], b2_ref[...]).astype(bf16)
    wide = D // TP
    for t in range(TP):
        enc[t] = last[:, t * wide : (t + 1) * wide]
    mine = pl.ds(tp * own_rows, own_rows)
    for i in range(1, TP):
        t = lax.rem(tp + i, TP)
        rc(enc.at[t], out_ref.at[mine, :], e_s, e_r, {"tp": t}).start()
    out_ref[mine, :] = enc[tp]

    sent(qb.at[pl.ds(0, NY - 1)], q_s)
    sent(wb.at[pl.ds(0, NY - 1), :, pl.ds(0, FA)], ya_s)
    sent(kvb.at[pl.ds(0, NZ - 1)], kv_s)
    sent(wb.at[pl.ds(0, (NZ - 1) * NY), :, pl.ds(0, FA)], wa_s)
    sent(wb.at[pl.ds(0, NZ - 1), :, pl.ds(FA, FW - FA)], wz_s)
    sent(wb.at[pl.ds(0, 3 * NZ), :, pl.ds(FA, FW - FA)], yf_s)
    sent(oms.at[pl.ds(0, NY * TP - 1)], o_s)
    sent(wo.at[pl.ds(0, NX)], wp_s)
    sent(xg.at[pl.ds(0, NX)], xp_s)
    sent(prb, p_s)
    if NX > 1:
        sent(wo.at[pl.ds(0, NX - 1)], wo_s)
        sent(xg.at[pl.ds(0, NX - 1)], x_s)
        sent(rr.at[:, pl.ds(0, NX - 1)], r_s)
    sent(enc.at[pl.ds(0, TP - 1)], e_s)
    got(out_ref.at[pl.ds(0, (TP - 1) * own_rows), :], e_r)


def solution(mesh):
    SP, TP = mesh.shape["sp"], mesh.shape["tp"]
    NZ, NX = SP // NY, TP // 2

    def local(queries, keys, values, q_gain, key_norm_gain, out_weight, residual, ln1_gain, ln1_bias, up_weight, down_weight, ln2_gain, ln2_bias):
        tok, D, FW = queries.shape[0], out_weight.shape[1], up_weight.shape[1]
        own = tok // TP
        FA = (FW // 128 * 3 // 8) * 128
        piece = up_weight.shape[0]
        rows, cols = rotary_tables(tok * SP, SP)
        quarters = 4
        vm, hbm = pl.BlockSpec(memory_space=pltpu.VMEM), pl.BlockSpec(memory_space=pl.ANY)
        dma = pltpu.SemaphoreType.DMA
        one = dma(())
        V = pltpu.VMEM
        flops = 2 * tok * tok * SP * 256 + 4 * tok * D * FW
        rs = (quarters, NX, own, D // quarters)
        return pl.pallas_call(
            functools.partial(kernel, NZ, NX, FA),
            out_shape=jax.ShapeDtypeStruct((tok, D // TP), bf16),
            in_specs=[vm, vm, vm, vm, vm, hbm, vm, hbm, hbm, hbm, hbm, vm, vm, vm, vm],
            out_specs=vm,
            scratch_shapes=[
                V(rows.shape[1:], f32), V((NY, tok, 128), bf16), V((NZ, tok, 128), bf16), V((NY * tok * 2, 128), bf16),
                V((NY * tok * 2, 128), f32), V((NY * tok * 2, 128), f32),
                V((SP, 2 * piece, FW), bf16), V((TP, 128, D), bf16),
                V((NY * TP, 2 * own, 128), bf16), V((NY * TP, 2 * own, 128), bf16), V((own, TP * 128), bf16),
                V((own, D), f32), V((own, D), bf16), V((TP, own, D), bf16), V((tok, FW), bf16),
                V((quarters, TP, own, D // quarters), bf16), V(rs, bf16), V(rs, bf16), V(rs, bf16), V((TP, own, D // TP), bf16),
                one, dma((NY,)), one, dma((NZ,)), one, dma((NZ, 2)), one, dma((NZ,)),
                one, dma((NY,)), one, dma((NZ, 2)), one, one, dma((2,)), one,
                one, one, one, dma((TP + 1,)), one,
                one, dma((quarters,)), one, dma((quarters,)), one, one, dma((5,)),
            ],
            compiler_params=pltpu.CompilerParams(collective_id=0, has_side_effects=True, vmem_limit_bytes=60000000),
            cost_estimate=pl.CostEstimate(flops=flops, bytes_accessed=30000000, transcendentals=0),
        )(
            queries, keys.T, values.T, q_gain[None], key_norm_gain[None], jnp.asarray(rows), jnp.asarray(cols),
            up_weight, down_weight.T, out_weight, residual, ln1_gain[None], ln1_bias[None], ln2_gain[None], ln2_bias[None],
        )

    return jax.shard_map(
        local,
        mesh=mesh,
        in_specs=(
            P("sp", "tp"), P("sp", "tp"), P("sp", "tp"), P(), P(), P("tp", None), P("sp", None),
            P(), P(), P("sp", "tp"), P("tp", "sp"), P(), P(),
        ),
        out_specs=P("sp", "tp"),
        check_vma=False,
    )
```

```python
import functools

import jax
import jax.numpy as jnp
import numpy as np
from jax import lax
from jax.experimental import pallas as pl
from jax.experimental.pallas import tpu as pltpu
from jax.sharding import PartitionSpec as P

HEAD = 64
GRID_W = 64
NY = 4
ALPHA = 8.0**0.25
ROTARY_BASE = 10000.0
RMS_EPSILON = 1e-06
NORM_EPSILON = 1e-05
LOG2E = 1.4426950408889634
f32, bf16 = jnp.float32, jnp.bfloat16


def rotary_tables(tokens, devices):
    lane = np.arange(2 * HEAD) % HEAD
    pos = lane % 32
    freq = ROTARY_BASE ** (-(pos % 16) / 16.0)

    def table(count, mine):
        angle = np.arange(count)[:, None] * freq[None, :]
        cos, sin = np.cos(angle) * mine, np.sin(angle) * mine
        return np.concatenate([cos, np.where(pos < 16, -sin, 0.0), np.where(pos >= 16, sin, 0.0)], 1).astype(np.float32)

    rows = table(tokens // GRID_W, lane < 32).reshape(devices, -1, 6 * HEAD)
    return np.pad(rows, ((0, 0), (0, -rows.shape[1] % 8), (0, 0))), table(GRID_W, lane >= 32)


def dot(a, b, dims=((1,), (0,))):
    return lax.dot_general(a, b, (dims, ((), ())), preferred_element_type=f32)


NT = ((1,), (1,))


def kernel(
    NZ, NX, FU, FD,
    q_hbm, k_hbm, v_hbm, gq_hbm, gk_hbm, row_ref, col_hbm, up_ref, down_ref, wo_own, res_ref, g1_ref, b1_ref, g2_ref, b2_ref,
    out_ref,
    q_ref, kv_ref, gq_ref, gk_ref, col_ref, ln, rowv, qb, kvb, qx, acc, mx, wb, wo, oms, omr, att, yb, res, xg, hid, part, prb, comb, rr, enc,
    q_s, q_r, kv_s, kv_r, wa_s, wa_r, wz_s, wz_r, ya_s, ya_r, yf_s, yf_r, yh_r, wo_s, wo_r, wp_s, o_s, o_r, x_s, x_r, xp_s,
    p_s, p_r, r_s, r_r, e_s, e_r, loc,
):
    TP = 2 * NX
    HALF = NZ // 2
    sp, tp = lax.axis_index("sp"), lax.axis_index("tp")
    z, y = sp // NY, lax.rem(sp, NY)
    x, core = tp // 2, lax.rem(tp, 2)
    zr, zl = lax.rem(z + 1, NZ), lax.rem(z + NZ - 1, NZ)
    yu, yd = lax.rem(y + 1, NY), lax.rem(y + NY - 1, NY)
    right, left = {"sp": zr * NY + y}, {"sp": zl * NY + y}
    above, below = {"sp": z * NY + yu}, {"sp": z * NY + yd}
    partner = {"tp": x * 2 + 1 - core}
    me = y * TP + tp
    tok = q_hbm.shape[0]
    own_rows = tok // TP
    D = wo.shape[2]
    FW = wb.shape[2]
    piece = up_ref.shape[0]

    def rc(src, dst, ss, rs, dev):
        return pltpu.make_async_remote_copy(
            src_ref=src, dst_ref=dst, send_sem=ss, recv_sem=rs, device_id=dev, device_id_type=pl.DeviceIdType.MESH
        )

    def got(ref, rs):
        rc(ref, ref, rs, rs, right).wait_recv()

    def sent(ref, ss):
        rc(ref, ref, ss, ss, right).wait_send()

    copies = [
        pltpu.make_async_copy(row_ref.at[sp], rowv, loc.at[0]),
        pltpu.make_async_copy(up_ref, wb.at[sp, pl.ds(0, piece), :], loc.at[1]),
        pltpu.make_async_copy(down_ref, wb.at[sp, pl.ds(piece, piece), :], loc.at[2]),
        pltpu.make_async_copy(wo_own, wo.at[tp], loc.at[3]),
        pltpu.make_async_copy(res_ref.at[pl.ds(tp * own_rows, own_rows), :], res, loc.at[4]),
    ]
    first = [
        pltpu.make_async_copy(k_hbm, kv_ref.at[pl.ds(0, HEAD), :], loc.at[5]),
        pltpu.make_async_copy(v_hbm, kv_ref.at[pl.ds(HEAD, HEAD), :], loc.at[6]),
        copies[0],
        pltpu.make_async_copy(col_hbm, col_ref, loc.at[7]),
        pltpu.make_async_copy(gk_hbm, gk_ref, loc.at[8]),
    ]
    second = [
        pltpu.make_async_copy(q_hbm, q_ref, loc.at[9]),
        pltpu.make_async_copy(gq_hbm, gq_ref, loc.at[10]),
    ]
    third = [pltpu.make_async_copy(r, ln.at[i], loc.at[11 + i]) for i, r in enumerate((g1_ref, b1_ref, g2_ref, b2_ref))]
    for c in first + second + copies[1:] + third:
        c.start()

    barrier = pltpu.get_barrier_semaphore()
    for dev in (right, left):
        pl.semaphore_signal(barrier, inc=1, device_id=dev, device_id_type=pl.DeviceIdType.MESH)

    @pl.loop(1, NY * TP)
    def _(i):
        d = lax.rem(me + i, NY * TP)
        pl.semaphore_signal(
            barrier, inc=1, device_id={"sp": z * NY + d // TP, "tp": lax.rem(d, TP)}, device_id_type=pl.DeviceIdType.MESH
        )

    lane = lax.broadcasted_iota(jnp.int32, (1, 2 * HEAD), 1)
    low = lane < HEAD
    for c in first:
        c.wait()
    kv_all = jnp.transpose(kv_ref[...].astype(f32))
    gk = jnp.concatenate([gk_ref[...], gk_ref[...]], 1)

    def spans():
        for r in range(tok // GRID_W):
            cs = [rowv[r : r + 1, 128 * k : 128 * (k + 1)] + col_ref[:, 128 * k : 128 * (k + 1)] for k in range(3)]
            yield pl.ds(r * GRID_W, GRID_W), cs, kv_all[r * GRID_W : (r + 1) * GRID_W]

    def turn(v, gain, cs):
        sq = v * v
        s0 = jnp.sum(jnp.where(low, sq, 0.0), -1, keepdims=True)
        s1 = jnp.sum(jnp.where(low, 0.0, sq), -1, keepdims=True)
        inv = jnp.where(low, lax.rsqrt(s0 / HEAD + RMS_EPSILON), lax.rsqrt(s1 / HEAD + RMS_EPSILON))
        n = v * inv * gain
        return n * cs[0] + pltpu.roll(n, 112, 1) * cs[1] + pltpu.roll(n, 16, 1) * cs[2]

    for span, cs, kv in spans():
        kvb[z, span, :] = jnp.where(low, turn(kv, gk, cs), kv).astype(bf16)

    pl.semaphore_wait(barrier, NY * TP + 1)

    cut = (FU, FD)

    def first_at(row, h):
        return wb.at[row, pl.ds(h * piece, piece), pl.ds(0, cut[h])]

    def half_at(slot, row, h):
        return wb.at[slot * NY + row, pl.ds(h * piece, piece), pl.ds(cut[h], FW - cut[h])]

    def amount(rows):
        return wb.at[pl.ds(0, rows), pl.ds(0, piece), pl.ds(0, FU + FD)]

    def halves(rows, h):
        return wb.at[pl.ds(0, rows), pl.ds(h * piece, piece), pl.ds(cut[h], FW - cut[h])]

    def send_kv(slot, dev):
        rc(kvb.at[slot], kvb.at[slot], kv_s, kv_r.at[slot], dev).start()

    def send_wa(slot, dev, k):
        for h in range(2):
            r = first_at(slot * NY + k, h)
            rc(r, r, wa_s, wa_r.at[slot, k], dev).start()

    def send_wz(slot, dev, h):
        rc(half_at(slot, y, h), half_at(slot, y, h), wz_s.at[h], wz_r.at[slot, h], dev).start()

    def minus(s):
        return lax.rem(z + NZ - s, NZ)

    def plus(s):
        return lax.rem(z + s, NZ)

    def both(s, ref, sem, send, send_first, send_last):
        def onward():
            send(minus(s), right)

        def last():
            send_first(minus(s), right)

        got(ref(minus(s)), sem.at[minus(s)])
        if isinstance(s, int):
            onward() if s < HALF - 1 else last()
        else:
            pl.when(s < HALF - 1)(onward)
            pl.when(s == HALF - 1)(last)
        got(ref(plus(s)), sem.at[plus(s)])
        if isinstance(s, int):
            send(plus(s), left) if s < HALF - 1 else send_last(plus(s), left)
        else:
            pl.when(s < HALF - 1)(lambda: send(plus(s), left))
            pl.when(s == HALF - 1)(lambda: send_last(plus(s), left))

    def step_kv(s):
        def part_of(lo):
            def f(i, dev):
                r = kvb.at[i, pl.ds(lo, tok // 2), :]
                rc(r, r, kv_s, kv_r.at[i], dev).start()

            return f

        both(s, lambda i: kvb.at[i], kv_r, send_kv, part_of(0), part_of(tok // 2))

    def nothing(i, dev):
        pass

    def step_wz(s):
        for h in range(2):

            def go(i, dev, h=h):
                send_wz(i, dev, h)

            both(s, lambda i, h=h: half_at(i, y, h), wz_r.at[:, h], go, nothing if h else go, go if h else nothing)

    def sub_wa(s, k):
        def go(i, dev):
            send_wa(i, dev, k)

        low_half = isinstance(k, int) and k < NY // 2
        both(s, lambda i: amount(1), wa_r.at[:, k], go, go if low_half else nothing, nothing if low_half else go)

    def step_wa(s):
        for k in range(NY):
            sub_wa(s, k)

    def spread(slot):
        for h, onward, last in ((0, above, below), (1, below, above)):
            r = half_at(slot, y, h)
            rc(r, r, yf_s.at[h], yf_r.at[slot, h], onward).start()
            rc(r, r, yf_s.at[h], yh_r.at[h], last).start()

    def relay(slot):
        for h, source, onward in ((0, yd, above), (1, yu, below)):
            r = half_at(slot, source, h)
            got(r, yf_r.at[slot, h])
            rc(r, r, yf_s.at[h], yh_r.at[h], onward).start()

    def pair(s, f):
        f(minus(s))
        f(plus(s))

    send_kv(z, right)
    send_kv(z, left)
    copies[1].wait()
    copies[2].wait()
    for i in range(1, NY):
        t = lax.rem(y + i, NY)
        for h in range(2):
            own = first_at(sp, h)
            rc(own, own, ya_s, ya_r.at[y], {"sp": z * NY + t}).start()
    for h in range(2):
        send_wz(z, right, h)
        send_wz(z, left, h)
    for c in second:
        c.wait()
    gq = jnp.concatenate([gq_ref[...], gq_ref[...]], 1) * (HEAD**-0.5 * LOG2E)
    for span, cs, kv in spans():
        qb[y, span, :] = turn(q_ref[span, :].astype(f32), gq, cs).astype(bf16)
    for i in range(1, NY):
        t = lax.rem(y + i, NY)
        rc(qb.at[y], qb.at[y], q_s, q_r.at[y], {"sp": z * NY + t}).start()
    spread(z)
    copies[3].wait()
    for i in range(1, NX):
        t = lax.rem(x + i, NX) * 2 + core
        rc(wo.at[tp], wo.at[tp], wo_s, wo_r.at[0], {"tp": t}).start()

    def spread_q(row):
        v = qb[row].astype(f32)
        h0 = jnp.where(low, v, 0.0).astype(bf16)
        h1 = jnp.where(low, pltpu.roll(v, HEAD, 1), 0.0).astype(bf16)
        for t in range(TP):
            at = (row * TP + t) * 2 * own_rows
            part_rows = slice(t * own_rows, (t + 1) * own_rows)
            qx[pl.ds(pl.multiple_of(at, own_rows), own_rows), :] = h0[part_rows]
            qx[pl.ds(pl.multiple_of(at + own_rows, own_rows), own_rows), :] = h1[part_rows]

    def flash(slots):
        kvs = [kvb[s] for s in slots]
        ones = [jnp.where(low, jnp.ones_like(k), k) for k in kvs]
        ss = [dot(qx[...], k, NT) for k in kvs]
        top = jnp.max(functools.reduce(jnp.maximum, ss), -1, keepdims=True)
        old = mx[...]
        new = jnp.maximum(old, top)
        wide = jnp.concatenate([new] * (tok // 128), 1) if tok > 128 else new[:, :tok]
        ps = [jnp.exp2(s - wide).astype(bf16) for s in ss]
        add = functools.reduce(jnp.add, [dot(p, v) for p, v in zip(ps, ones)])
        acc[...] = acc[...] * jnp.exp2(old - new) + add
        mx[...] = new

    acc[...] = jnp.zeros_like(acc)
    mx[...] = jnp.full_like(mx, -1e30)
    spread_q(y)
    beside = HALF - 2
    SM = HALF - 3

    @pl.loop(1, HALF)
    def _(s):
        step_kv(s)
        step_wz(s)

        @pl.when(s == 1)
        def _():
            for i in range(1, NY):
                t = lax.rem(y + i, NY)
                got(amount(1), ya_r.at[t])
            for k in range(NY):
                send_wa(z, right, k)
                send_wa(z, left, k)
            for i in range(1, NY):
                t = lax.rem(y + i, NY)
                got(qb.at[t], q_r.at[t])
                spread_q(t)
            flash([z])

        @pl.when(s > 1)
        def _():
            sub_wa((s - 2) // NY + 1, lax.rem(s - 2, NY))

        @pl.when(s <= SM)
        def _():
            pair(s, spread)

        flash([minus(s), plus(s)])

        @pl.when((s >= 2) & (s <= SM + 2))
        def _():
            relay(minus(s - 2))

            @pl.when(s > 2)
            def _():
                relay(plus(s - 2))

    far = lax.rem(z + HALF, NZ)
    for i in range(beside, -(-beside // NY) * NY):
        sub_wa(i // NY + 1, i % NY)
    rest = list(range(-(-beside // NY) + 1, HALF))
    got(kvb.at[far], kv_r.at[far])
    flash([far])

    o = (acc[...] / pltpu.roll(acc[...], HEAD, 1)).reshape(NY * TP, 2, own_rows, 128)
    heads = jnp.where(low, pltpu.roll(o[:, 0].reshape(-1, 128), HEAD, 1), o[:, 1].reshape(-1, 128))
    oms[:, :own_rows, :] = heads.astype(bf16).reshape(NY * TP, own_rows, 128)
    lse = (mx[...] + jnp.log2(acc[...])).reshape(NY * TP, 2 * own_rows, 128)
    at = lax.broadcasted_iota(jnp.int32, lse.shape, 1) == lax.broadcasted_iota(jnp.int32, lse.shape, 2)
    lse = jnp.sum(jnp.where(at, lse, 0.0), 1, keepdims=True)
    hi = lse.astype(bf16).astype(f32)
    mid = (lse - hi).astype(bf16).astype(f32)
    row = lax.broadcasted_iota(jnp.int32, (NY * TP, 16, 128), 1)
    parts = jnp.where(row == 0, hi, jnp.where(row == 1, mid, jnp.where(row == 2, lse - hi - mid, 0.0)))
    oms[:, own_rows:, :] = parts.astype(bf16)

    @pl.loop(1, NY * TP)
    def _(i):
        d = lax.rem(me + i, NY * TP)
        rc(oms.at[d], omr.at[me], o_s, o_r, {"sp": z * NY + d // TP, "tp": lax.rem(d, TP)}).start()

    omr[me] = oms[me]
    for s in rest[:1]:
        step_wa(s)
    for s in range(SM + 1, HALF - 1):
        pair(s, spread)
    if NX > 1:
        got(wo.at[pl.ds(0, NX - 1)], wo_r.at[0])
    for i in range(NX):
        t = lax.rem(x + i, NX) * 2 + core
        rc(wo.at[t], wo.at[t], wp_s, wo_r.at[1], partner).start()
    for h in range(2):
        got(half_at(far, y, h), wz_r.at[far, h])
    for s in rest[1:2]:
        step_wa(s)
    pair(HALF - 1, spread)
    got(omr.at[pl.ds(0, NY * TP - 1)], o_r)

    @pl.loop(0, TP)
    def _(t):
        msgs = [omr[r * TP + t].astype(f32) for r in range(NY)]
        row = lax.broadcasted_iota(jnp.int32, (own_rows, 128), 0)
        lses = []
        for m in msgs:
            line = jnp.sum(m[own_rows:], 0, keepdims=True)
            h0, h1 = (jnp.sum(jnp.where(row + at == lane, line, 0.0), -1, keepdims=True) for at in (0, own_rows))
            lses.append(jnp.where(low, h0, h1))
        top = functools.reduce(jnp.maximum, lses)
        ws = [jnp.exp2(v - top) for v in lses]
        o = functools.reduce(jnp.add, [w * m[:own_rows] for w, m in zip(ws, msgs)]) / functools.reduce(jnp.add, ws)
        att[:, pl.ds(pl.multiple_of(t * 128, 128), 128)] = o.astype(bf16)

    got(wo.at[pl.ds(0, NX)], wo_r.at[1])
    copies[4].wait()
    for c in third:
        c.wait()

    CW = min(1024, D)

    @pl.loop(0, D // CW)
    def _(n):
        cols = pl.ds(pl.multiple_of(n * CW, CW), CW)
        w = wo[:, :, cols].reshape(TP * 128, CW)
        yb[:, cols] = dot(att[...], w) + ALPHA * res[:, cols].astype(f32)

    def norm(v, gain, bias):
        mean = jnp.mean(v, -1, keepdims=True)
        c = v - mean
        return c * lax.rsqrt(jnp.mean(c * c, -1, keepdims=True) + NORM_EPSILON) * gain + bias

    xg[tp] = norm(yb[...], ln[0], ln[1]).astype(bf16)
    for i in range(1, NX):
        t = lax.rem(x + i, NX) * 2 + core
        rc(xg.at[tp], xg.at[tp], x_s, x_r.at[tp], {"tp": t}).start()
    rc(xg.at[tp], xg.at[tp], xp_s, x_r.at[TP], partner).start()
    late = list(range(SM + 1, HALF))
    for s in rest[2:]:
        step_wa(s)
        if s == rest[2]:
            spread(far)
        if late and s < HALF - 1:
            pair(late.pop(0), relay)
    if not rest[2:]:
        spread(far)
    for s in late:
        pair(s, relay)
    relay(far)
    for i in range(1, NX):
        t = lax.rem(x + i, NX) * 2 + core
        got(xg.at[t], x_r.at[t])
        rc(xg.at[t], xg.at[t], xp_s, x_r.at[TP], partner).start()
    for k in range(NY):
        got(amount(1), wa_r.at[far, k])
    got(xg.at[pl.ds(0, NX)], x_r.at[TP])
    for h in range(2):
        got(halves(2 * NZ, h), yh_r.at[h])

    up = dot(xg[...].reshape(tok, D), wb[:, :piece, :].reshape(D, FW))
    hid[...] = jnp.square(jnp.maximum(up, 0.0)).astype(bf16)

    QW = part.shape[3]
    quarters = D // QW
    per = QW // piece

    def down(h):
        w = wb[pl.ds(h * per, per), piece:, :].reshape(QW, FW)
        part[h] = dot(hid[...], w, NT).astype(bf16).reshape(TP, own_rows, QW)
        for i in range(1, NX + 1):
            t = lax.rem(x + i, NX)
            rc(part.at[h, t * 2 + 1 - core], prb.at[h, t], p_s, p_r.at[h], partner).start()

    def fold(h):
        got(prb.at[h], p_r.at[h])
        for i in range(1, NX):
            t = lax.rem(x + i, NX)
            comb[h, t] = (part[h, t * 2 + core].astype(f32) + prb[h, t].astype(f32)).astype(bf16)
            rc(comb.at[h, t], rr.at[h, x], r_s, r_r.at[h], {"tp": t * 2 + core}).start()

    for h in range(quarters):
        down(h)
        if h > 0:
            fold(h - 1)
    fold(quarters - 1)
    for h in range(quarters):
        cols = slice(h * QW, (h + 1) * QW)
        total = part[h, tp].astype(f32) + prb[h, x].astype(f32) + ALPHA * xg[tp, :, cols].astype(f32)
        if NX > 1:
            got(rr.at[h, pl.ds(0, NX - 1)], r_r.at[h])
            for i in range(1, NX):
                total += rr[h, lax.rem(x + i, NX)].astype(f32)
        yb[:, cols] = total
    last = norm(yb[...], ln[2], ln[3]).astype(bf16)
    wide = D // TP
    for t in range(TP):
        enc[t] = last[:, t * wide : (t + 1) * wide]
    mine = pl.ds(tp * own_rows, own_rows)
    for i in range(1, TP):
        t = lax.rem(tp + i, TP)
        rc(enc.at[t], out_ref.at[mine, :], e_s, e_r, {"tp": t}).start()
    out_copy = pltpu.make_async_copy(enc.at[tp], out_ref.at[mine, :], loc.at[15])
    out_copy.start()

    sent(qb.at[pl.ds(0, NY - 1)], q_s)
    sent(amount(NY - 1), ya_s)
    sent(kvb.at[pl.ds(0, NZ - 1)], kv_s)
    sent(amount((NZ - 1) * NY), wa_s)
    for h in range(2):
        sent(halves(NZ - 1, h), wz_s.at[h])
        sent(halves(3 * NZ, h), yf_s.at[h])
    sent(oms.at[pl.ds(0, NY * TP - 1)], o_s)
    sent(wo.at[pl.ds(0, NX)], wp_s)
    sent(xg.at[pl.ds(0, NX)], xp_s)
    sent(prb, p_s)
    if NX > 1:
        sent(wo.at[pl.ds(0, NX - 1)], wo_s)
        sent(xg.at[pl.ds(0, NX - 1)], x_s)
        sent(rr.at[:, pl.ds(0, NX - 1)], r_s)
    sent(enc.at[pl.ds(0, TP - 1)], e_s)
    out_copy.wait()
    got(out_ref.at[pl.ds(0, (TP - 1) * own_rows), :], e_r)


def solution(mesh):
    SP, TP = mesh.shape["sp"], mesh.shape["tp"]
    NZ, NX = SP // NY, TP // 2

    def local(queries, keys, values, q_gain, key_norm_gain, out_weight, residual, ln1_gain, ln1_bias, up_weight, down_weight, ln2_gain, ln2_bias):
        tok, D, FW = queries.shape[0], out_weight.shape[1], up_weight.shape[1]
        own = tok // TP
        FU, FD = FW // 1024 * 384, FW // 1024 * 384
        piece = up_weight.shape[0]
        rows, cols = rotary_tables(tok * SP, SP)
        quarters = 4
        hbm = pl.BlockSpec(memory_space=pl.ANY)
        dma = pltpu.SemaphoreType.DMA
        one = dma(())
        V = pltpu.VMEM
        flops = 2 * tok * tok * SP * 256 + 4 * tok * D * FW
        rs = (quarters, NX, own, D // quarters)
        return pl.pallas_call(
            functools.partial(kernel, NZ, NX, FU, FD),
            out_shape=jax.ShapeDtypeStruct((tok, D // TP), bf16),
            in_specs=[hbm] * 15,
            out_specs=hbm,
            scratch_shapes=[
                V((tok, 128), bf16), V((2 * HEAD, tok), bf16), V((1, HEAD), f32), V((1, HEAD), f32), V(cols.shape, f32), V((4, 1, D), f32),
                V(rows.shape[1:], f32), V((NY, tok, 128), bf16), V((NZ, tok, 128), bf16), V((NY * tok * 2, 128), bf16),
                V((NY * tok * 2, 128), f32), V((NY * tok * 2, 128), f32),
                V((SP, 2 * piece, FW), bf16), V((TP, 128, D), bf16),
                V((NY * TP, own + 16, 128), bf16), V((NY * TP, own + 16, 128), bf16), V((own, TP * 128), bf16),
                V((own, D), f32), V((own, D), bf16), V((TP, own, D), bf16), V((tok, FW), bf16),
                V((quarters, TP, own, D // quarters), bf16), V(rs, bf16), V(rs, bf16), V(rs, bf16), V((TP, own, D // TP), bf16),
                one, dma((NY,)), one, dma((NZ,)), one, dma((NZ, NY)), dma((2,)), dma((NZ, 2)),
                one, dma((NY,)), dma((2,)), dma((NZ, 2)), dma((2,)), one, dma((2,)), one,
                one, one, one, dma((TP + 1,)), one,
                one, dma((quarters,)), one, dma((quarters,)), one, one, dma((16,)),
            ],
            compiler_params=pltpu.CompilerParams(collective_id=0, has_side_effects=True, vmem_limit_bytes=60000000),
            cost_estimate=pl.CostEstimate(flops=flops, bytes_accessed=30000000, transcendentals=0),
        )(
            queries, keys.T, values.T, q_gain[None], key_norm_gain[None], jnp.asarray(rows), jnp.asarray(cols),
            up_weight, down_weight.T, out_weight, residual, ln1_gain[None], ln1_bias[None], ln2_gain[None], ln2_bias[None],
        )

    return jax.shard_map(
        local,
        mesh=mesh,
        in_specs=(
            P("sp", "tp"), P("sp", "tp"), P("sp", "tp"), P(), P(), P("tp", None), P("sp", None),
            P(), P(), P("sp", "tp"), P("tp", "sp"), P(), P(),
        ),
        out_specs=P("sp", "tp"),
        check_vma=False,
    )
```

```python
import functools

import jax
import jax.numpy as jnp
import numpy as np
from jax import lax
from jax.experimental import pallas as pl
from jax.experimental.pallas import tpu as pltpu
from jax.sharding import PartitionSpec as P

HEAD = 64
GRID_W = 64
NY = 4
ALPHA = 8.0**0.25
ROTARY_BASE = 10000.0
RMS_EPSILON = 1e-06
NORM_EPSILON = 1e-05
LOG2E = 1.4426950408889634
f32, bf16 = jnp.float32, jnp.bfloat16


def rotary_tables(tokens, devices):
    lane = np.arange(2 * HEAD) % HEAD
    pos = lane % 32
    freq = ROTARY_BASE ** (-(pos % 16) / 16.0)

    def table(count, mine):
        angle = np.arange(count)[:, None] * freq[None, :]
        cos, sin = np.cos(angle) * mine, np.sin(angle) * mine
        return np.concatenate([cos, np.where(pos < 16, -sin, 0.0), np.where(pos >= 16, sin, 0.0)], 1).astype(np.float32)

    rows = table(tokens // GRID_W, lane < 32).reshape(devices, -1, 6 * HEAD)
    return np.pad(rows, ((0, 0), (0, -rows.shape[1] % 8), (0, 0))), table(GRID_W, lane >= 32)


def dot(a, b, dims=((1,), (0,))):
    return lax.dot_general(a, b, (dims, ((), ())), preferred_element_type=f32)


NT = ((1,), (1,))


def kernel(
    NZ, NX, FU, FD,
    q_hbm, k_hbm, v_hbm, gq_hbm, gk_hbm, row_ref, col_hbm, up_ref, down_ref, wo_own, res_ref, g1_ref, b1_ref, g2_ref, b2_ref,
    out_ref,
    q_ref, kv_ref, gq_ref, gk_ref, col_ref, ln, rowv, qb, kvb, qx, acc, mx, wb, wo, oms, omr, att, yb, res, xg, hid, part, prb, comb, rr, enc,
    q_s, q_r, kv_s, kv_r, wa_s, wa_r, wz_s, wz_r, ya_s, ya_r, yf_s, yf_r, yh_r, wo_s, wo_r, wp_s, o_s, o_r, x_s, x_r, xp_s,
    p_s, p_r, r_s, r_r, e_s, e_r, loc,
):
    TP = 2 * NX
    HALF = NZ // 2
    sp, tp = lax.axis_index("sp"), lax.axis_index("tp")
    z, y = sp // NY, lax.rem(sp, NY)
    x, core = tp // 2, lax.rem(tp, 2)
    zr, zl = lax.rem(z + 1, NZ), lax.rem(z + NZ - 1, NZ)
    yu, yd = lax.rem(y + 1, NY), lax.rem(y + NY - 1, NY)
    right, left = {"sp": zr * NY + y}, {"sp": zl * NY + y}
    above, below = {"sp": z * NY + yu}, {"sp": z * NY + yd}
    partner = {"tp": x * 2 + 1 - core}
    me = y * TP + tp
    tok = q_hbm.shape[0]
    own_rows = tok // TP
    D = wo.shape[2]
    FW = wb.shape[2]
    piece = up_ref.shape[0]

    def rc(src, dst, ss, rs, dev):
        return pltpu.make_async_remote_copy(
            src_ref=src, dst_ref=dst, send_sem=ss, recv_sem=rs, device_id=dev, device_id_type=pl.DeviceIdType.MESH
        )

    def got(ref, rs):
        rc(ref, ref, rs, rs, right).wait_recv()

    def sent(ref, ss):
        rc(ref, ref, ss, ss, right).wait_send()

    copies = [
        pltpu.make_async_copy(row_ref.at[sp], rowv, loc.at[0]),
        pltpu.make_async_copy(up_ref, wb.at[sp, pl.ds(0, piece), :], loc.at[1]),
        pltpu.make_async_copy(down_ref, wb.at[sp, pl.ds(piece, piece), :], loc.at[2]),
        pltpu.make_async_copy(wo_own, wo.at[tp], loc.at[3]),
        pltpu.make_async_copy(res_ref.at[pl.ds(tp * own_rows, own_rows), :], res, loc.at[4]),
    ]
    first = [
        pltpu.make_async_copy(k_hbm, kv_ref.at[pl.ds(0, HEAD), :], loc.at[5]),
        pltpu.make_async_copy(v_hbm, kv_ref.at[pl.ds(HEAD, HEAD), :], loc.at[6]),
        copies[0],
        pltpu.make_async_copy(col_hbm, col_ref, loc.at[7]),
        pltpu.make_async_copy(gk_hbm, gk_ref, loc.at[8]),
    ]
    second = [
        pltpu.make_async_copy(q_hbm, q_ref, loc.at[9]),
        pltpu.make_async_copy(gq_hbm, gq_ref, loc.at[10]),
    ]
    third = [pltpu.make_async_copy(r, ln.at[i], loc.at[11 + i]) for i, r in enumerate((g1_ref, b1_ref, g2_ref, b2_ref))]
    for c in first + second + copies[1:] + third:
        c.start()

    barrier = pltpu.get_barrier_semaphore()
    for dev in (right, left):
        pl.semaphore_signal(barrier, inc=1, device_id=dev, device_id_type=pl.DeviceIdType.MESH)

    @pl.loop(1, NY * TP)
    def _(i):
        d = lax.rem(me + i, NY * TP)
        pl.semaphore_signal(
            barrier, inc=1, device_id={"sp": z * NY + d // TP, "tp": lax.rem(d, TP)}, device_id_type=pl.DeviceIdType.MESH
        )

    lane = lax.broadcasted_iota(jnp.int32, (1, 2 * HEAD), 1)
    low = lane < HEAD
    for c in first:
        c.wait()
    kv_all = jnp.transpose(kv_ref[...].astype(f32))
    gk = jnp.concatenate([gk_ref[...], gk_ref[...]], 1)

    def spans():
        for r in range(tok // GRID_W):
            cs = [rowv[r : r + 1, 128 * k : 128 * (k + 1)] + col_ref[:, 128 * k : 128 * (k + 1)] for k in range(3)]
            yield pl.ds(r * GRID_W, GRID_W), cs, kv_all[r * GRID_W : (r + 1) * GRID_W]

    def turn(v, gain, cs):
        sq = v * v
        s0 = jnp.sum(jnp.where(low, sq, 0.0), -1, keepdims=True)
        s1 = jnp.sum(jnp.where(low, 0.0, sq), -1, keepdims=True)
        inv = jnp.where(low, lax.rsqrt(s0 / HEAD + RMS_EPSILON), lax.rsqrt(s1 / HEAD + RMS_EPSILON))
        n = v * inv * gain
        return n * cs[0] + pltpu.roll(n, 112, 1) * cs[1] + pltpu.roll(n, 16, 1) * cs[2]

    for span, cs, kv in spans():
        kvb[z, span, :] = jnp.where(low, turn(kv, gk, cs), kv).astype(bf16)

    pl.semaphore_wait(barrier, NY * TP + 1)

    cut = (FU, FD)

    def first_at(row, h):
        return wb.at[row, pl.ds(h * piece, piece), pl.ds(0, cut[h])]

    def half_at(slot, row, h):
        return wb.at[slot * NY + row, pl.ds(h * piece, piece), pl.ds(cut[h], FW - cut[h])]

    def amount(rows):
        return wb.at[pl.ds(0, rows), pl.ds(0, piece), pl.ds(0, FU + FD)]

    def halves(rows, h):
        return wb.at[pl.ds(0, rows), pl.ds(h * piece, piece), pl.ds(cut[h], FW - cut[h])]

    def send_kv(slot, dev):
        rc(kvb.at[slot], kvb.at[slot], kv_s, kv_r.at[slot], dev).start()

    def send_wa(slot, dev, k):
        for h in range(2):
            r = first_at(slot * NY + k, h)
            rc(r, r, wa_s, wa_r.at[slot, k], dev).start()

    def send_wz(slot, dev, h):
        rc(half_at(slot, y, h), half_at(slot, y, h), wz_s.at[h], wz_r.at[slot, h], dev).start()

    def minus(s):
        return lax.rem(z + NZ - s, NZ)

    def plus(s):
        return lax.rem(z + s, NZ)

    def both(s, ref, sem, send, send_first, send_last):
        def onward():
            send(minus(s), right)

        def last():
            send_first(minus(s), right)

        got(ref(minus(s)), sem.at[minus(s)])
        if isinstance(s, int):
            onward() if s < HALF - 1 else last()
        else:
            pl.when(s < HALF - 1)(onward)
            pl.when(s == HALF - 1)(last)
        got(ref(plus(s)), sem.at[plus(s)])
        if isinstance(s, int):
            send(plus(s), left) if s < HALF - 1 else send_last(plus(s), left)
        else:
            pl.when(s < HALF - 1)(lambda: send(plus(s), left))
            pl.when(s == HALF - 1)(lambda: send_last(plus(s), left))

    def step_kv(s):
        def part_of(lo):
            def f(i, dev):
                r = kvb.at[i, pl.ds(lo, tok // 2), :]
                rc(r, r, kv_s, kv_r.at[i], dev).start()

            return f

        both(s, lambda i: kvb.at[i], kv_r, send_kv, part_of(0), part_of(tok // 2))

    def nothing(i, dev):
        pass

    def step_wz(s):
        for h in range(2):

            def go(i, dev, h=h):
                send_wz(i, dev, h)

            both(s, lambda i, h=h: half_at(i, y, h), wz_r.at[:, h], go, nothing if h else go, go if h else nothing)

    def sub_wa(s, k):
        other = (k + NY // 2) % NY if isinstance(k, int) else lax.rem(k + NY // 2, NY)
        got(amount(1), wa_r.at[minus(s), k])
        if not isinstance(s, int) or s < HALF - 1 or k < NY // 2:
            send_wa(minus(s), right, k)
        got(amount(1), wa_r.at[plus(s), other])
        if not isinstance(s, int) or s < HALF - 1 or k < NY // 2:
            send_wa(plus(s), left, other)

    def step_wa(s):
        for k in range(NY):
            sub_wa(s, k)

    def spread(slot):
        for h, onward, last in ((0, above, below), (1, below, above)):
            r = half_at(slot, y, h)
            rc(r, r, yf_s.at[h], yf_r.at[slot, h], onward).start()
            rc(r, r, yf_s.at[h], yh_r.at[h], last).start()

    def relay(slot):
        for h, source, onward in ((0, yd, above), (1, yu, below)):
            r = half_at(slot, source, h)
            got(r, yf_r.at[slot, h])
            rc(r, r, yf_s.at[h], yh_r.at[h], onward).start()

    def pair(s, f):
        f(minus(s))
        f(plus(s))

    send_kv(z, right)
    send_kv(z, left)
    copies[1].wait()
    copies[2].wait()
    for i in range(1, NY):
        t = lax.rem(y + i, NY)
        for h in range(2):
            own = first_at(sp, h)
            rc(own, own, ya_s, ya_r.at[y], {"sp": z * NY + t}).start()
    for h in range(2):
        send_wz(z, right, h)
        send_wz(z, left, h)
    for c in second:
        c.wait()
    gq = jnp.concatenate([gq_ref[...], gq_ref[...]], 1) * (HEAD**-0.5 * LOG2E)
    for span, cs, kv in spans():
        qb[y, span, :] = turn(q_ref[span, :].astype(f32), gq, cs).astype(bf16)
    for i in range(1, NY):
        t = lax.rem(y + i, NY)
        rc(qb.at[y], qb.at[y], q_s, q_r.at[y], {"sp": z * NY + t}).start()
    spread(z)
    copies[3].wait()
    for i in range(1, NX):
        t = lax.rem(x + i, NX) * 2 + core
        rc(wo.at[tp], wo.at[tp], wo_s, wo_r.at[0], {"tp": t}).start()

    def spread_q(row):
        v = qb[row].astype(f32)
        h0 = jnp.where(low, v, 0.0).astype(bf16)
        h1 = jnp.where(low, pltpu.roll(v, HEAD, 1), 0.0).astype(bf16)
        for t in range(TP):
            at = (row * TP + t) * 2 * own_rows
            part_rows = slice(t * own_rows, (t + 1) * own_rows)
            qx[pl.ds(pl.multiple_of(at, own_rows), own_rows), :] = h0[part_rows]
            qx[pl.ds(pl.multiple_of(at + own_rows, own_rows), own_rows), :] = h1[part_rows]

    def flash(slots):
        kvs = [kvb[s] for s in slots]
        ones = [jnp.where(low, jnp.ones_like(k), k) for k in kvs]
        ss = [dot(qx[...], k, NT) for k in kvs]
        top = jnp.max(functools.reduce(jnp.maximum, ss), -1, keepdims=True)
        old = mx[...]
        new = jnp.maximum(old, top)
        wide = jnp.concatenate([new] * (tok // 128), 1) if tok > 128 else new[:, :tok]
        ps = [jnp.exp2(s - wide).astype(bf16) for s in ss]
        add = functools.reduce(jnp.add, [dot(p, v) for p, v in zip(ps, ones)])
        acc[...] = acc[...] * jnp.exp2(old - new) + add
        mx[...] = new

    acc[...] = jnp.zeros_like(acc)
    mx[...] = jnp.full_like(mx, -1e30)
    spread_q(y)
    beside = HALF - 2
    SM = HALF - 3

    @pl.loop(1, HALF)
    def _(s):
        step_kv(s)
        step_wz(s)

        @pl.when(s == 1)
        def _():
            for i in range(1, NY):
                t = lax.rem(y + i, NY)
                got(amount(1), ya_r.at[t])
            for k in range(NY):
                send_wa(z, right, k)
                send_wa(z, left, (k + NY // 2) % NY)
            for i in range(1, NY):
                t = lax.rem(y + i, NY)
                got(qb.at[t], q_r.at[t])
                spread_q(t)
            flash([z])

        @pl.when(s > 1)
        def _():
            sub_wa((s - 2) // NY + 1, lax.rem(s - 2, NY))

        @pl.when(s <= SM)
        def _():
            pair(s, spread)

        flash([minus(s), plus(s)])

        @pl.when((s >= 2) & (s <= SM + 2))
        def _():
            relay(minus(s - 2))

            @pl.when(s > 2)
            def _():
                relay(plus(s - 2))

    far = lax.rem(z + HALF, NZ)
    for i in range(beside, -(-beside // NY) * NY):
        sub_wa(i // NY + 1, i % NY)
    rest = list(range(-(-beside // NY) + 1, HALF))
    got(kvb.at[far], kv_r.at[far])
    flash([far])

    o = (acc[...] / pltpu.roll(acc[...], HEAD, 1)).reshape(NY * TP, 2, own_rows, 128)
    heads = jnp.where(low, pltpu.roll(o[:, 0].reshape(-1, 128), HEAD, 1), o[:, 1].reshape(-1, 128))
    oms[:, :own_rows, :] = heads.astype(bf16).reshape(NY * TP, own_rows, 128)
    lse = (mx[...] + jnp.log2(acc[...])).reshape(NY * TP, 2 * own_rows, 128)
    at = lax.broadcasted_iota(jnp.int32, lse.shape, 1) == lax.broadcasted_iota(jnp.int32, lse.shape, 2)
    lse = jnp.sum(jnp.where(at, lse, 0.0), 1, keepdims=True)
    hi = lse.astype(bf16).astype(f32)
    mid = (lse - hi).astype(bf16).astype(f32)
    row = lax.broadcasted_iota(jnp.int32, (NY * TP, 16, 128), 1)
    parts = jnp.where(row == 0, hi, jnp.where(row == 1, mid, jnp.where(row == 2, lse - hi - mid, 0.0)))
    oms[:, own_rows:, :] = parts.astype(bf16)

    @pl.loop(1, NY * TP)
    def _(i):
        d = lax.rem(me + i, NY * TP)
        rc(oms.at[d], omr.at[me], o_s, o_r, {"sp": z * NY + d // TP, "tp": lax.rem(d, TP)}).start()

    omr[me] = oms[me]
    for s in rest[:1]:
        step_wa(s)
    for s in range(SM + 1, HALF - 1):
        pair(s, spread)
    if NX > 1:
        got(wo.at[pl.ds(0, NX - 1)], wo_r.at[0])
    for i in range(NX):
        t = lax.rem(x + i, NX) * 2 + core
        rc(wo.at[t], wo.at[t], wp_s, wo_r.at[1], partner).start()
    for h in range(2):
        got(half_at(far, y, h), wz_r.at[far, h])
    for s in rest[1:2]:
        step_wa(s)
    pair(HALF - 1, spread)
    got(omr.at[pl.ds(0, NY * TP - 1)], o_r)

    @pl.loop(0, TP)
    def _(t):
        msgs = [omr[r * TP + t].astype(f32) for r in range(NY)]
        row = lax.broadcasted_iota(jnp.int32, (own_rows, 128), 0)
        lses = []
        for m in msgs:
            line = jnp.sum(m[own_rows:], 0, keepdims=True)
            h0, h1 = (jnp.sum(jnp.where(row + at == lane, line, 0.0), -1, keepdims=True) for at in (0, own_rows))
            lses.append(jnp.where(low, h0, h1))
        top = functools.reduce(jnp.maximum, lses)
        ws = [jnp.exp2(v - top) for v in lses]
        o = functools.reduce(jnp.add, [w * m[:own_rows] for w, m in zip(ws, msgs)]) / functools.reduce(jnp.add, ws)
        att[:, pl.ds(pl.multiple_of(t * 128, 128), 128)] = o.astype(bf16)

    got(wo.at[pl.ds(0, NX)], wo_r.at[1])
    copies[4].wait()
    for c in third:
        c.wait()

    CW = min(1024, D)

    @pl.loop(0, D // CW)
    def _(n):
        cols = pl.ds(pl.multiple_of(n * CW, CW), CW)
        w = wo[:, :, cols].reshape(TP * 128, CW)
        yb[:, cols] = dot(att[...], w) + ALPHA * res[:, cols].astype(f32)

    def norm(v, gain, bias):
        mean = jnp.mean(v, -1, keepdims=True)
        c = v - mean
        return c * lax.rsqrt(jnp.mean(c * c, -1, keepdims=True) + NORM_EPSILON) * gain + bias

    xg[tp] = norm(yb[...], ln[0], ln[1]).astype(bf16)
    for i in range(1, NX):
        t = lax.rem(x + i, NX) * 2 + core
        rc(xg.at[tp], xg.at[tp], x_s, x_r.at[tp], {"tp": t}).start()
    rc(xg.at[tp], xg.at[tp], xp_s, x_r.at[TP], partner).start()
    late = list(range(SM + 1, HALF))
    relayed = False
    for s in rest[2:]:
        step_wa(s)
        if s == rest[2]:
            spread(far)
        if late and s < HALF - 1:
            pair(late.pop(0), relay)
        if s == HALF - 2:
            for k in late:
                pair(k, relay)
            late = []
            relay(far)
            relayed = True
    if not rest[2:]:
        spread(far)
    for s in late:
        pair(s, relay)
    if not relayed:
        relay(far)
    for i in range(1, NX):
        t = lax.rem(x + i, NX) * 2 + core
        got(xg.at[t], x_r.at[t])
        rc(xg.at[t], xg.at[t], xp_s, x_r.at[TP], partner).start()
    for k in range(NY):
        got(amount(1), wa_r.at[far, k])
    got(xg.at[pl.ds(0, NX)], x_r.at[TP])
    for h in range(2):
        got(halves(2 * NZ, h), yh_r.at[h])

    up = dot(xg[...].reshape(tok, D), wb[:, :piece, :].reshape(D, FW))
    hid[...] = jnp.square(jnp.maximum(up, 0.0)).astype(bf16)

    QW = part.shape[3]
    quarters = D // QW
    per = QW // piece

    def down(h):
        w = wb[pl.ds(h * per, per), piece:, :].reshape(QW, FW)
        part[h] = dot(hid[...], w, NT).astype(bf16).reshape(TP, own_rows, QW)
        for i in range(1, NX + 1):
            t = lax.rem(x + i, NX)
            rc(part.at[h, t * 2 + 1 - core], prb.at[h, t], p_s, p_r.at[h], partner).start()

    def fold(h):
        got(prb.at[h], p_r.at[h])
        for i in range(1, NX):
            t = lax.rem(x + i, NX)
            comb[h, t] = (part[h, t * 2 + core].astype(f32) + prb[h, t].astype(f32)).astype(bf16)
            rc(comb.at[h, t], rr.at[h, x], r_s, r_r.at[h], {"tp": t * 2 + core}).start()

    for h in range(quarters):
        down(h)
        if h > 0:
            fold(h - 1)
    fold(quarters - 1)
    for h in range(quarters):
        cols = slice(h * QW, (h + 1) * QW)
        total = part[h, tp].astype(f32) + prb[h, x].astype(f32) + ALPHA * xg[tp, :, cols].astype(f32)
        if NX > 1:
            got(rr.at[h, pl.ds(0, NX - 1)], r_r.at[h])
            for i in range(1, NX):
                total += rr[h, lax.rem(x + i, NX)].astype(f32)
        yb[:, cols] = total
    last = norm(yb[...], ln[2], ln[3]).astype(bf16)
    wide = D // TP
    for t in range(TP):
        enc[t] = last[:, t * wide : (t + 1) * wide]
    mine = pl.ds(tp * own_rows, own_rows)
    for i in range(1, TP):
        t = lax.rem(tp + i, TP)
        rc(enc.at[t], out_ref.at[mine, :], e_s, e_r, {"tp": t}).start()
    out_copy = pltpu.make_async_copy(enc.at[tp], out_ref.at[mine, :], loc.at[15])
    out_copy.start()

    sent(qb.at[pl.ds(0, NY - 1)], q_s)
    sent(amount(NY - 1), ya_s)
    sent(kvb.at[pl.ds(0, NZ - 1)], kv_s)
    sent(amount((NZ - 1) * NY), wa_s)
    for h in range(2):
        sent(halves(NZ - 1, h), wz_s.at[h])
        sent(halves(3 * NZ, h), yf_s.at[h])
    sent(oms.at[pl.ds(0, NY * TP - 1)], o_s)
    sent(wo.at[pl.ds(0, NX)], wp_s)
    sent(xg.at[pl.ds(0, NX)], xp_s)
    sent(prb, p_s)
    if NX > 1:
        sent(wo.at[pl.ds(0, NX - 1)], wo_s)
        sent(xg.at[pl.ds(0, NX - 1)], x_s)
        sent(rr.at[:, pl.ds(0, NX - 1)], r_s)
    sent(enc.at[pl.ds(0, TP - 1)], e_s)
    out_copy.wait()
    got(out_ref.at[pl.ds(0, (TP - 1) * own_rows), :], e_r)


def solution(mesh):
    SP, TP = mesh.shape["sp"], mesh.shape["tp"]
    NZ, NX = SP // NY, TP // 2

    def local(queries, keys, values, q_gain, key_norm_gain, out_weight, residual, ln1_gain, ln1_bias, up_weight, down_weight, ln2_gain, ln2_bias):
        tok, D, FW = queries.shape[0], out_weight.shape[1], up_weight.shape[1]
        own = tok // TP
        FU, FD = FW // 1024 * 384, FW // 1024 * 384
        piece = up_weight.shape[0]
        rows, cols = rotary_tables(tok * SP, SP)
        quarters = 4
        hbm = pl.BlockSpec(memory_space=pl.ANY)
        dma = pltpu.SemaphoreType.DMA
        one = dma(())
        V = pltpu.VMEM
        flops = 2 * tok * tok * SP * 256 + 4 * tok * D * FW
        rs = (quarters, NX, own, D // quarters)
        return pl.pallas_call(
            functools.partial(kernel, NZ, NX, FU, FD),
            out_shape=pltpu.VMEM((tok, D // TP), bf16),
            in_specs=[hbm] * 15,
            out_specs=pl.BlockSpec(memory_space=pltpu.VMEM),
            scratch_shapes=[
                V((tok, 128), bf16), V((2 * HEAD, tok), bf16), V((1, HEAD), f32), V((1, HEAD), f32), V(cols.shape, f32), V((4, 1, D), f32),
                V(rows.shape[1:], f32), V((NY, tok, 128), bf16), V((NZ, tok, 128), bf16), V((NY * tok * 2, 128), bf16),
                V((NY * tok * 2, 128), f32), V((NY * tok * 2, 128), f32),
                V((SP, 2 * piece, FW), bf16), V((TP, 128, D), bf16),
                V((NY * TP, own + 16, 128), bf16), V((NY * TP, own + 16, 128), bf16), V((own, TP * 128), bf16),
                V((own, D), f32), V((own, D), bf16), V((TP, own, D), bf16), V((tok, FW), bf16),
                V((quarters, TP, own, D // quarters), bf16), V(rs, bf16), V(rs, bf16), V(rs, bf16), V((TP, own, D // TP), bf16),
                one, dma((NY,)), one, dma((NZ,)), one, dma((NZ, NY)), dma((2,)), dma((NZ, 2)),
                one, dma((NY,)), dma((2,)), dma((NZ, 2)), dma((2,)), one, dma((2,)), one,
                one, one, one, dma((TP + 1,)), one,
                one, dma((quarters,)), one, dma((quarters,)), one, one, dma((16,)),
            ],
            compiler_params=pltpu.CompilerParams(collective_id=0, has_side_effects=True, vmem_limit_bytes=60000000),
            cost_estimate=pl.CostEstimate(flops=flops, bytes_accessed=30000000, transcendentals=0),
        )(
            queries, keys.T, values.T, q_gain[None], key_norm_gain[None], jnp.asarray(rows), jnp.asarray(cols),
            up_weight, down_weight.T, out_weight, residual, ln1_gain[None], ln1_bias[None], ln2_gain[None], ln2_bias[None],
        )

    return jax.shard_map(
        local,
        mesh=mesh,
        in_specs=(
            P("sp", "tp"), P("sp", "tp"), P("sp", "tp"), P(), P(), P("tp", None), P("sp", None),
            P(), P(), P("sp", "tp"), P("tp", "sp"), P(), P(),
        ),
        out_specs=P("sp", "tp"),
        check_vma=False,
    )
```

```python
import functools

import jax
import jax.numpy as jnp
import numpy as np
from jax import lax
from jax.experimental import pallas as pl
from jax.experimental.pallas import tpu as pltpu
from jax.sharding import PartitionSpec as P

HEAD = 64
GRID_W = 64
NY = 4
ALPHA = 8.0**0.25
ROTARY_BASE = 10000.0
RMS_EPSILON = 1e-06
NORM_EPSILON = 1e-05
LOG2E = 1.4426950408889634
f32, bf16 = jnp.float32, jnp.bfloat16


def rotary_tables(tokens, devices):
    lane = np.arange(2 * HEAD) % HEAD
    pos = lane % 32
    freq = ROTARY_BASE ** (-(pos % 16) / 16.0)

    def table(count, mine):
        angle = np.arange(count)[:, None] * freq[None, :]
        cos, sin = np.cos(angle) * mine, np.sin(angle) * mine
        return np.concatenate([cos, np.where(pos < 16, -sin, 0.0), np.where(pos >= 16, sin, 0.0)], 1).astype(np.float32)

    rows = table(tokens // GRID_W, lane < 32).reshape(devices, -1, 6 * HEAD)
    return np.pad(rows, ((0, 0), (0, -rows.shape[1] % 8), (0, 0))), table(GRID_W, lane >= 32)


def dot(a, b, dims=((1,), (0,))):
    return lax.dot_general(a, b, (dims, ((), ())), preferred_element_type=f32)


NT = ((1,), (1,))


def kernel(
    NZ, NX, FU, FD,
    q_hbm, k_hbm, v_hbm, gq_hbm, gk_hbm, row_ref, col_hbm, up_ref, down_ref, wo_own, res_ref, g1_ref, b1_ref, g2_ref, b2_ref,
    out_ref,
    q_ref, kv_ref, gq_ref, gk_ref, col_ref, ln, rowv, qb, kvb, qx, acc, mx, wb, wo, oms, omr, att, yb, res, xg, hid, part, prb, comb, rr, enc,
    q_s, q_r, kv_s, kv_r, wa_s, wa_r, wz_s, wz_r, ya_s, ya_r, yf_s, yf_r, yh_r, wo_s, wo_r, wp_s, o_s, o_r, x_s, x_r, xp_s,
    p_s, p_r, r_s, r_r, e_s, e_r, loc, left_in,
):
    TP = 2 * NX
    HALF = NZ // 2
    sp, tp = lax.axis_index("sp"), lax.axis_index("tp")
    z, y = sp // NY, lax.rem(sp, NY)
    x, core = tp // 2, lax.rem(tp, 2)
    zr, zl = lax.rem(z + 1, NZ), lax.rem(z + NZ - 1, NZ)
    yu, yd = lax.rem(y + 1, NY), lax.rem(y + NY - 1, NY)
    right, left = {"sp": zr * NY + y}, {"sp": zl * NY + y}
    above, below = {"sp": z * NY + yu}, {"sp": z * NY + yd}
    partner = {"tp": x * 2 + 1 - core}
    me = y * TP + tp
    tok = q_hbm.shape[0]
    own_rows = tok // TP
    D = wo.shape[2]
    FW = wb.shape[2]
    piece = up_ref.shape[0]

    def rc(src, dst, ss, rs, dev):
        return pltpu.make_async_remote_copy(
            src_ref=src, dst_ref=dst, send_sem=ss, recv_sem=rs, device_id=dev, device_id_type=pl.DeviceIdType.MESH
        )

    def got(ref, rs):
        rc(ref, ref, rs, rs, right).wait_recv()

    def sent(ref, ss):
        rc(ref, ref, ss, ss, right).wait_send()

    copies = [
        pltpu.make_async_copy(row_ref.at[sp], rowv, loc.at[0]),
        pltpu.make_async_copy(up_ref, wb.at[sp, pl.ds(0, piece), :], loc.at[1]),
        pltpu.make_async_copy(down_ref, wb.at[sp, pl.ds(piece, piece), :], loc.at[2]),
        pltpu.make_async_copy(wo_own, wo.at[tp], loc.at[3]),
        pltpu.make_async_copy(res_ref.at[pl.ds(tp * own_rows, own_rows), :], res, loc.at[4]),
    ]
    first = [
        pltpu.make_async_copy(k_hbm, kv_ref.at[pl.ds(0, HEAD), :], loc.at[5]),
        pltpu.make_async_copy(v_hbm, kv_ref.at[pl.ds(HEAD, HEAD), :], loc.at[6]),
        copies[0],
        pltpu.make_async_copy(col_hbm, col_ref, loc.at[7]),
        pltpu.make_async_copy(gk_hbm, gk_ref, loc.at[8]),
    ]
    second = [
        pltpu.make_async_copy(q_hbm, q_ref, loc.at[9]),
        pltpu.make_async_copy(gq_hbm, gq_ref, loc.at[10]),
    ]
    third = [pltpu.make_async_copy(r, ln.at[i], loc.at[11 + i]) for i, r in enumerate((g1_ref, b1_ref, g2_ref, b2_ref))]
    for c in first + second + copies[1:] + third:
        c.start()

    barrier = pltpu.get_barrier_semaphore()
    pl.semaphore_signal(barrier, inc=1, device_id=left, device_id_type=pl.DeviceIdType.MESH)

    @pl.loop(1, NY * TP)
    def _(i):
        d = lax.rem(me + i, NY * TP)
        pl.semaphore_signal(
            barrier, inc=1, device_id={"sp": z * NY + d // TP, "tp": lax.rem(d, TP)}, device_id_type=pl.DeviceIdType.MESH
        )

    lane = lax.broadcasted_iota(jnp.int32, (1, 2 * HEAD), 1)
    low = lane < HEAD
    for c in first:
        c.wait()
    kv_all = jnp.transpose(kv_ref[...].astype(f32))
    gk = jnp.concatenate([gk_ref[...], gk_ref[...]], 1)

    def spans():
        for r in range(tok // GRID_W):
            cs = [rowv[r : r + 1, 128 * k : 128 * (k + 1)] + col_ref[:, 128 * k : 128 * (k + 1)] for k in range(3)]
            yield pl.ds(r * GRID_W, GRID_W), cs, kv_all[r * GRID_W : (r + 1) * GRID_W]

    def turn(v, gain, cs):
        sq = v * v
        s0 = jnp.sum(jnp.where(low, sq, 0.0), -1, keepdims=True)
        s1 = jnp.sum(jnp.where(low, 0.0, sq), -1, keepdims=True)
        inv = jnp.where(low, lax.rsqrt(s0 / HEAD + RMS_EPSILON), lax.rsqrt(s1 / HEAD + RMS_EPSILON))
        n = v * inv * gain
        return n * cs[0] + pltpu.roll(n, 112, 1) * cs[1] + pltpu.roll(n, 16, 1) * cs[2]

    for span, cs, kv in spans():
        kvb[z, span, :] = jnp.where(low, turn(kv, gk, cs), kv).astype(bf16)

    pl.semaphore_wait(barrier, NY * TP)
    pl.semaphore_signal(left_in, inc=1, device_id=right, device_id_type=pl.DeviceIdType.MESH)

    cut = (FU, FD)

    def first_at(row, h):
        return wb.at[row, pl.ds(h * piece, piece), pl.ds(0, cut[h])]

    def half_at(slot, row, h):
        return wb.at[slot * NY + row, pl.ds(h * piece, piece), pl.ds(cut[h], FW - cut[h])]

    def amount(rows):
        return wb.at[pl.ds(0, rows), pl.ds(0, piece), pl.ds(0, FU + FD)]

    def halves(rows, h):
        return wb.at[pl.ds(0, rows), pl.ds(h * piece, piece), pl.ds(cut[h], FW - cut[h])]

    def send_kv(slot, dev):
        rc(kvb.at[slot], kvb.at[slot], kv_s, kv_r.at[slot], dev).start()

    def send_wa(slot, dev, k):
        for h in range(2):
            r = first_at(slot * NY + k, h)
            rc(r, r, wa_s, wa_r.at[slot, k], dev).start()

    def send_wz(slot, dev, h):
        rc(half_at(slot, y, h), half_at(slot, y, h), wz_s.at[h], wz_r.at[slot, h], dev).start()

    def minus(s):
        return lax.rem(z + NZ - s, NZ)

    def plus(s):
        return lax.rem(z + s, NZ)

    def both(s, ref, sem, send, send_first, send_last):
        def onward():
            send(minus(s), right)

        def last():
            send_first(minus(s), right)

        got(ref(minus(s)), sem.at[minus(s)])
        if isinstance(s, int):
            onward() if s < HALF - 1 else last()
        else:
            pl.when(s < HALF - 1)(onward)
            pl.when(s == HALF - 1)(last)
        got(ref(plus(s)), sem.at[plus(s)])
        if isinstance(s, int):
            send(plus(s), left) if s < HALF - 1 else send_last(plus(s), left)
        else:
            pl.when(s < HALF - 1)(lambda: send(plus(s), left))
            pl.when(s == HALF - 1)(lambda: send_last(plus(s), left))

    def step_kv(s):
        def part_of(lo):
            def f(i, dev):
                r = kvb.at[i, pl.ds(lo, tok // 2), :]
                rc(r, r, kv_s, kv_r.at[i], dev).start()

            return f

        both(s, lambda i: kvb.at[i], kv_r, send_kv, part_of(0), part_of(tok // 2))

    def nothing(i, dev):
        pass

    def step_wz(s):
        for h in range(2):

            def go(i, dev, h=h):
                send_wz(i, dev, h)

            both(s, lambda i, h=h: half_at(i, y, h), wz_r.at[:, h], go, nothing if h else go, go if h else nothing)

    def sub_wa(s, k):
        other = (k + NY // 2) % NY if isinstance(k, int) else lax.rem(k + NY // 2, NY)
        got(amount(1), wa_r.at[minus(s), k])
        if not isinstance(s, int) or s < HALF - 1 or k < NY // 2:
            send_wa(minus(s), right, k)
        got(amount(1), wa_r.at[plus(s), other])
        if not isinstance(s, int) or s < HALF - 1 or k < NY // 2:
            send_wa(plus(s), left, other)

    def step_wa(s):
        for k in range(NY):
            sub_wa(s, k)

    def spread(slot):
        for h, onward, last in ((0, above, below), (1, below, above)):
            r = half_at(slot, y, h)
            rc(r, r, yf_s.at[h], yf_r.at[slot, h], onward).start()
            rc(r, r, yf_s.at[h], yh_r.at[h], last).start()

    def relay(slot):
        for h, source, onward in ((0, yd, above), (1, yu, below)):
            r = half_at(slot, source, h)
            got(r, yf_r.at[slot, h])
            rc(r, r, yf_s.at[h], yh_r.at[h], onward).start()

    def pair(s, f):
        f(minus(s))
        f(plus(s))

    send_kv(z, right)
    copies[1].wait()
    copies[2].wait()
    for i in range(1, NY):
        t = lax.rem(y + i, NY)
        for h in range(2):
            own = first_at(sp, h)
            rc(own, own, ya_s, ya_r.at[y], {"sp": z * NY + t}).start()
    for h in range(2):
        send_wz(z, right, h)
    pl.semaphore_wait(left_in, 1)
    send_kv(z, left)
    for h in range(2):
        send_wz(z, left, h)
    for c in second:
        c.wait()
    gq = jnp.concatenate([gq_ref[...], gq_ref[...]], 1) * (HEAD**-0.5 * LOG2E)
    for span, cs, kv in spans():
        qb[y, span, :] = turn(q_ref[span, :].astype(f32), gq, cs).astype(bf16)
    for i in range(1, NY):
        t = lax.rem(y + i, NY)
        rc(qb.at[y], qb.at[y], q_s, q_r.at[y], {"sp": z * NY + t}).start()
    spread(z)
    copies[3].wait()
    for i in range(1, NX):
        t = lax.rem(x + i, NX) * 2 + core
        rc(wo.at[tp], wo.at[tp], wo_s, wo_r.at[0], {"tp": t}).start()

    def spread_q(row):
        v = qb[row].astype(f32)
        h0 = jnp.where(low, v, 0.0).astype(bf16)
        h1 = jnp.where(low, pltpu.roll(v, HEAD, 1), 0.0).astype(bf16)
        for t in range(TP):
            at = (row * TP + t) * 2 * own_rows
            part_rows = slice(t * own_rows, (t + 1) * own_rows)
            qx[pl.ds(pl.multiple_of(at, own_rows), own_rows), :] = h0[part_rows]
            qx[pl.ds(pl.multiple_of(at + own_rows, own_rows), own_rows), :] = h1[part_rows]

    def flash(slots):
        kvs = [kvb[s] for s in slots]
        ones = [jnp.where(low, jnp.ones_like(k), k) for k in kvs]
        ss = [dot(qx[...], k, NT) for k in kvs]
        top = jnp.max(functools.reduce(jnp.maximum, ss), -1, keepdims=True)
        old = mx[...]
        new = jnp.maximum(old, top)
        wide = jnp.concatenate([new] * (tok // 128), 1) if tok > 128 else new[:, :tok]
        ps = [jnp.exp2(s - wide).astype(bf16) for s in ss]
        add = functools.reduce(jnp.add, [dot(p, v) for p, v in zip(ps, ones)])
        acc[...] = acc[...] * jnp.exp2(old - new) + add
        mx[...] = new

    acc[...] = jnp.zeros_like(acc)
    mx[...] = jnp.full_like(mx, -1e30)
    spread_q(y)
    beside = HALF - 2
    SM = HALF - 3

    @pl.loop(1, HALF)
    def _(s):
        step_kv(s)
        step_wz(s)

        @pl.when(s == 1)
        def _():
            for i in range(1, NY):
                t = lax.rem(y + i, NY)
                got(amount(1), ya_r.at[t])
            for k in range(NY):
                send_wa(z, right, k)
                send_wa(z, left, (k + NY // 2) % NY)
            for i in range(1, NY):
                t = lax.rem(y + i, NY)
                got(qb.at[t], q_r.at[t])
                spread_q(t)
            flash([z])

        @pl.when(s > 1)
        def _():
            sub_wa((s - 2) // NY + 1, lax.rem(s - 2, NY))

        @pl.when(s <= SM)
        def _():
            pair(s, spread)

        flash([minus(s), plus(s)])

        @pl.when((s >= 2) & (s <= SM + 2))
        def _():
            relay(minus(s - 2))

            @pl.when(s > 2)
            def _():
                relay(plus(s - 2))

    far = lax.rem(z + HALF, NZ)
    for i in range(beside, -(-beside // NY) * NY):
        sub_wa(i // NY + 1, i % NY)
    rest = list(range(-(-beside // NY) + 1, HALF))
    got(kvb.at[far], kv_r.at[far])
    flash([far])

    o = (acc[...] / pltpu.roll(acc[...], HEAD, 1)).reshape(NY * TP, 2, own_rows, 128)
    heads = jnp.where(low, pltpu.roll(o[:, 0].reshape(-1, 128), HEAD, 1), o[:, 1].reshape(-1, 128))
    oms[:, :own_rows, :] = heads.astype(bf16).reshape(NY * TP, own_rows, 128)
    lse = (mx[...] + jnp.log2(acc[...])).reshape(NY * TP, 2 * own_rows, 128)
    at = lax.broadcasted_iota(jnp.int32, lse.shape, 1) == lax.broadcasted_iota(jnp.int32, lse.shape, 2)
    lse = jnp.sum(jnp.where(at, lse, 0.0), 1, keepdims=True)
    hi = lse.astype(bf16).astype(f32)
    mid = (lse - hi).astype(bf16).astype(f32)
    row = lax.broadcasted_iota(jnp.int32, (NY * TP, 16, 128), 1)
    parts = jnp.where(row == 0, hi, jnp.where(row == 1, mid, jnp.where(row == 2, lse - hi - mid, 0.0)))
    oms[:, own_rows:, :] = parts.astype(bf16)

    @pl.loop(1, NY * TP)
    def _(i):
        d = lax.rem(me + i, NY * TP)
        rc(oms.at[d], omr.at[me], o_s, o_r, {"sp": z * NY + d // TP, "tp": lax.rem(d, TP)}).start()

    omr[me] = oms[me]
    for s in rest[:1]:
        step_wa(s)
    for s in range(SM + 1, HALF - 1):
        pair(s, spread)
    if NX > 1:
        got(wo.at[pl.ds(0, NX - 1)], wo_r.at[0])
    for i in range(NX):
        t = lax.rem(x + i, NX) * 2 + core
        rc(wo.at[t], wo.at[t], wp_s, wo_r.at[1], partner).start()
    for h in range(2):
        got(half_at(far, y, h), wz_r.at[far, h])
    for s in rest[1:2]:
        step_wa(s)
    pair(HALF - 1, spread)
    got(omr.at[pl.ds(0, NY * TP - 1)], o_r)

    @pl.loop(0, TP)
    def _(t):
        msgs = [omr[r * TP + t].astype(f32) for r in range(NY)]
        row = lax.broadcasted_iota(jnp.int32, (own_rows, 128), 0)
        lses = []
        for m in msgs:
            line = jnp.sum(m[own_rows:], 0, keepdims=True)
            h0, h1 = (jnp.sum(jnp.where(row + at == lane, line, 0.0), -1, keepdims=True) for at in (0, own_rows))
            lses.append(jnp.where(low, h0, h1))
        top = functools.reduce(jnp.maximum, lses)
        ws = [jnp.exp2(v - top) for v in lses]
        o = functools.reduce(jnp.add, [w * m[:own_rows] for w, m in zip(ws, msgs)]) / functools.reduce(jnp.add, ws)
        att[:, pl.ds(pl.multiple_of(t * 128, 128), 128)] = o.astype(bf16)

    got(wo.at[pl.ds(0, NX)], wo_r.at[1])
    copies[4].wait()
    for c in third:
        c.wait()

    CW = min(1024, D)

    @pl.loop(0, D // CW)
    def _(n):
        cols = pl.ds(pl.multiple_of(n * CW, CW), CW)
        w = wo[:, :, cols].reshape(TP * 128, CW)
        yb[:, cols] = dot(att[...], w) + ALPHA * res[:, cols].astype(f32)

    def norm(v, gain, bias):
        mean = jnp.mean(v, -1, keepdims=True)
        c = v - mean
        return c * lax.rsqrt(jnp.mean(c * c, -1, keepdims=True) + NORM_EPSILON) * gain + bias

    xg[tp] = norm(yb[...], ln[0], ln[1]).astype(bf16)
    for i in range(1, NX):
        t = lax.rem(x + i, NX) * 2 + core
        rc(xg.at[tp], xg.at[tp], x_s, x_r.at[tp], {"tp": t}).start()
    rc(xg.at[tp], xg.at[tp], xp_s, x_r.at[TP], partner).start()
    late = list(range(SM + 1, HALF))
    relayed = False
    for s in rest[2:]:
        step_wa(s)
        if s == rest[2]:
            spread(far)
        if late and s < HALF - 1:
            pair(late.pop(0), relay)
        if s == HALF - 2:
            for k in late:
                pair(k, relay)
            late = []
            relay(far)
            relayed = True
    if not rest[2:]:
        spread(far)
    for s in late:
        pair(s, relay)
    if not relayed:
        relay(far)
    for i in range(1, NX):
        t = lax.rem(x + i, NX) * 2 + core
        got(xg.at[t], x_r.at[t])
        rc(xg.at[t], xg.at[t], xp_s, x_r.at[TP], partner).start()
    for k in range(NY):
        got(amount(1), wa_r.at[far, k])
    got(xg.at[pl.ds(0, NX)], x_r.at[TP])
    for h in range(2):
        got(halves(2 * NZ, h), yh_r.at[h])

    up = dot(xg[...].reshape(tok, D), wb[:, :piece, :].reshape(D, FW))
    hid[...] = jnp.square(jnp.maximum(up, 0.0)).astype(bf16)

    QW = part.shape[3]
    quarters = D // QW
    per = QW // piece

    def down(h):
        w = wb[pl.ds(h * per, per), piece:, :].reshape(QW, FW)
        part[h] = dot(hid[...], w, NT).astype(bf16).reshape(TP, own_rows, QW)
        for i in range(1, NX + 1):
            t = lax.rem(x + i, NX)
            rc(part.at[h, t * 2 + 1 - core], prb.at[h, t], p_s, p_r.at[h], partner).start()

    def fold(h):
        got(prb.at[h], p_r.at[h])
        for i in range(1, NX):
            t = lax.rem(x + i, NX)
            comb[h, t] = (part[h, t * 2 + core].astype(f32) + prb[h, t].astype(f32)).astype(bf16)
            rc(comb.at[h, t], rr.at[h, x], r_s, r_r.at[h], {"tp": t * 2 + core}).start()

    for h in range(quarters):
        down(h)
        if h > 0:
            fold(h - 1)
    fold(quarters - 1)
    for h in range(quarters):
        cols = slice(h * QW, (h + 1) * QW)
        total = part[h, tp].astype(f32) + prb[h, x].astype(f32) + ALPHA * xg[tp, :, cols].astype(f32)
        if NX > 1:
            got(rr.at[h, pl.ds(0, NX - 1)], r_r.at[h])
            for i in range(1, NX):
                total += rr[h, lax.rem(x + i, NX)].astype(f32)
        yb[:, cols] = total
    last = norm(yb[...], ln[2], ln[3]).astype(bf16)
    wide = D // TP
    for t in range(TP):
        enc[t] = last[:, t * wide : (t + 1) * wide]
    mine = pl.ds(tp * own_rows, own_rows)
    for i in range(1, TP):
        t = lax.rem(tp + i, TP)
        rc(enc.at[t], out_ref.at[mine, :], e_s, e_r, {"tp": t}).start()
    out_copy = pltpu.make_async_copy(enc.at[tp], out_ref.at[mine, :], loc.at[15])
    out_copy.start()

    sent(qb.at[pl.ds(0, NY - 1)], q_s)
    sent(amount(NY - 1), ya_s)
    sent(kvb.at[pl.ds(0, NZ - 1)], kv_s)
    sent(amount((NZ - 1) * NY), wa_s)
    for h in range(2):
        sent(halves(NZ - 1, h), wz_s.at[h])
        sent(halves(3 * NZ, h), yf_s.at[h])
    sent(oms.at[pl.ds(0, NY * TP - 1)], o_s)
    sent(wo.at[pl.ds(0, NX)], wp_s)
    sent(xg.at[pl.ds(0, NX)], xp_s)
    sent(prb, p_s)
    if NX > 1:
        sent(wo.at[pl.ds(0, NX - 1)], wo_s)
        sent(xg.at[pl.ds(0, NX - 1)], x_s)
        sent(rr.at[:, pl.ds(0, NX - 1)], r_s)
    sent(enc.at[pl.ds(0, TP - 1)], e_s)
    out_copy.wait()
    got(out_ref.at[pl.ds(0, (TP - 1) * own_rows), :], e_r)


def solution(mesh):
    SP, TP = mesh.shape["sp"], mesh.shape["tp"]
    NZ, NX = SP // NY, TP // 2

    def local(queries, keys, values, q_gain, key_norm_gain, out_weight, residual, ln1_gain, ln1_bias, up_weight, down_weight, ln2_gain, ln2_bias):
        tok, D, FW = queries.shape[0], out_weight.shape[1], up_weight.shape[1]
        own = tok // TP
        FU, FD = FW // 1024 * 384, FW // 1024 * 384
        piece = up_weight.shape[0]
        rows, cols = rotary_tables(tok * SP, SP)
        quarters = 4
        hbm = pl.BlockSpec(memory_space=pl.ANY)
        dma = pltpu.SemaphoreType.DMA
        one = dma(())
        V = pltpu.VMEM
        flops = 2 * tok * tok * SP * 256 + 4 * tok * D * FW
        rs = (quarters, NX, own, D // quarters)
        return pl.pallas_call(
            functools.partial(kernel, NZ, NX, FU, FD),
            out_shape=pltpu.VMEM((tok, D // TP), bf16),
            in_specs=[hbm] * 15,
            out_specs=pl.BlockSpec(memory_space=pltpu.VMEM),
            scratch_shapes=[
                V((tok, 128), bf16), V((2 * HEAD, tok), bf16), V((1, HEAD), f32), V((1, HEAD), f32), V(cols.shape, f32), V((4, 1, D), f32),
                V(rows.shape[1:], f32), V((NY, tok, 128), bf16), V((NZ, tok, 128), bf16), V((NY * tok * 2, 128), bf16),
                V((NY * tok * 2, 128), f32), V((NY * tok * 2, 128), f32),
                V((SP, 2 * piece, FW), bf16), V((TP, 128, D), bf16),
                V((NY * TP, own + 16, 128), bf16), V((NY * TP, own + 16, 128), bf16), V((own, TP * 128), bf16),
                V((own, D), f32), V((own, D), bf16), V((TP, own, D), bf16), V((tok, FW), bf16),
                V((quarters, TP, own, D // quarters), bf16), V(rs, bf16), V(rs, bf16), V(rs, bf16), V((TP, own, D // TP), bf16),
                one, dma((NY,)), one, dma((NZ,)), one, dma((NZ, NY)), dma((2,)), dma((NZ, 2)),
                one, dma((NY,)), dma((2,)), dma((NZ, 2)), dma((2,)), one, dma((2,)), one,
                one, one, one, dma((TP + 1,)), one,
                one, dma((quarters,)), one, dma((quarters,)), one, one, dma((16,)), pltpu.SemaphoreType.REGULAR,
            ],
            compiler_params=pltpu.CompilerParams(collective_id=0, has_side_effects=True, vmem_limit_bytes=60000000),
            cost_estimate=pl.CostEstimate(flops=flops, bytes_accessed=30000000, transcendentals=0),
        )(
            queries, keys.T, values.T, q_gain[None], key_norm_gain[None], jnp.asarray(rows), jnp.asarray(cols),
            up_weight, down_weight.T, out_weight, residual, ln1_gain[None], ln1_bias[None], ln2_gain[None], ln2_bias[None],
        )

    return jax.shard_map(
        local,
        mesh=mesh,
        in_specs=(
            P("sp", "tp"), P("sp", "tp"), P("sp", "tp"), P(), P(), P("tp", None), P("sp", None),
            P(), P(), P("sp", "tp"), P("tp", "sp"), P(), P(),
        ),
        out_specs=P("sp", "tp"),
        check_vma=False,
    )
```
